256 devices in a mesh: grp: 2 (over z), ep: 64 (over y, x), tp: 2 (over core).
Axes of the slice: x: 8, y: 8, z: 2, core: 2. Of those that a mesh axis runs over, the one named last changes fastest.
The devices are a block of a 8x8x16 slice.
Arguments:
- layer_input: bfloat16 [4096, 2048], P(('grp', 'ep')), parts along dimension 0, may hold values from -6 to 6
- ssm_state: float32 [2, 4096, 32, 64], P(None, ('grp', 'ep'), 'tp'), parts along dimension 1, may hold values from -4 to 4
- w_input: bfloat16 [2048, 512], P(None, 'tp'), may hold values from -0.125 to 0.125
- decay_rate: float32 [32, 64], P('tp'), may hold values from 0.05 to 2
- frequency: float32 [32, 64], P('tp'), may hold values from 0 to 20
- step_log: float32 [32], P('tp'), may hold values from -2.3 to 0
- input_map: float32 [2, 32, 64, 16], P(None, 'tp'), may hold values from -1 to 1
- output_map: float32 [2, 32, 16, 64], P(None, 'tp'), may hold values from -0.75 to 0.75
- skip_gain: float32 [32, 16], P('tp'), may hold values from -3 to 3
- glu_weight: bfloat16 [512, 512], replicated, may hold values from -0.25 to 0.25
- mix_out: bfloat16 [512, 2048], replicated, may hold values from -0.75 to 0.75
- norm_gain: float32 [2048], replicated, may hold values from 0.1 to 6, as said below
- norm_shift: float32 [2048], replicated, may hold values from -2 to 2
- route_ids: int32 [4096, 6], P(('grp', 'ep')), parts along dimension 0, may hold values from 0 to 63, all different within a row; in each aligned block of 32 rows (0 to 31, 32 to 63, ...) at most 6 rows name the same one
- route_weights: float32 [4096, 6], P(('grp', 'ep')), parts along dimension 0, may hold values from 0.1 to 1
- gate_expert: bfloat16 [64, 2048, 512], P('ep', None, 'tp'), may hold values from -0.125 to 0.125
- up_expert: bfloat16 [64, 2048, 512], P('ep', None, 'tp'), may hold values from -0.125 to 0.125
- down_expert: bfloat16 [64, 512, 2048], P('ep', 'tp'), may hold values from -0.25 to 0.25
- gate_shared: bfloat16 [2048, 512], P(None, 'tp'), may hold values from -0.125 to 0.125
- up_shared: bfloat16 [2048, 512], P(None, 'tp'), may hold values from -0.125 to 0.125
- down_shared: bfloat16 [512, 2048], P('tp'), may hold values from -0.25 to 0.25
- dense_in: bfloat16 [1024, 2048], P('ep'), may hold values from -0.125 to 0.125
- dense_out: bfloat16 [1024, 2048], P('ep', 'tp'), may hold values from -0.1875 to 0.1875
- branch_gate: bfloat16 [2048], replicated, may hold values from -0.125 to 0.125
- final_gain: float32 [2048], P('tp'), may hold values from 0.1 to 1.9
- final_shift: float32 [2048], P('tp'), may hold values from -2 to 2
Outputs:
- layer_output: bfloat16 [4096, 2048], P(('grp', 'ep'), 'tp'), parts along dimension 0
- new_state: float32 [2, 4096, 32, 64], P(None, ('grp', 'ep'), 'tp'), parts along dimension 1
The draws below stay inside these ranges and needn't reach their ends.
There are 2 independent parts, one for each index of `grp`. The reference program is written for one: setup_inputs(seed, part) draws one part's arguments, and reference() takes and returns one part's arrays. A program takes and returns all parts, laid end to end along the dimension named above; an argument that names none is the same for every part. Nothing has to cross between parts.
Inputs may be any that keep to these rules, and one draw needn't show every extreme that they name: `route_ids`: each row names 6 different experts; within each aligned block of 32 rows no expert is named more than 6 times, and in some block one expert is named exactly 6 times. `norm_gain`: positive gains.
All inputs are finite; a program needn't handle non-finite values.
Results may differ from the reference program's by a relative error of at most 0.015.
Values may be sent and summed in bfloat16 or wider, within the bound.
A program may use at most 128 MiB of HBM per device.

```python
import math
import jax
import jax.numpy as jnp
import numpy as np
from jax import lax

D = 2048
S5_WIDTH = 512
GROUP = 16
STATE = 64
EFF = 512
DENSE = 1024
TOP_K = 6
SEQ_DEV = 32
GROUPS = 32
EXPERTS = 64
SEQS = 2048
CAP = 6
N_EP = 64
N_TP = 2


def draw_norm_gain(key, part):
    ramp = jnp.arange(D, dtype=jnp.float32) / D
    base = jnp.exp(math.log(0.3) + math.log(10.0) * ramp)
    noise = jax.random.uniform(jax.random.fold_in(key, 11), (D,), jnp.float32, 0.7, 1.3)
    return jnp.clip(base * noise, 0.1, 6.0).astype(jnp.float32)


def levels(own_key, dims, cuts, low, top_value):
    level = 1.0
    for axis_at, parts in cuts:
        draws = jax.random.uniform(jax.random.fold_in(jax.random.fold_in(own_key, 6), axis_at), (parts,), jnp.float32, low / len(cuts), top_value / len(cuts))
        level = level * jnp.repeat(jnp.exp(draws), dims[axis_at] // parts).reshape((-1,) + (1,) * (len(dims) - 1 - axis_at))
    return level


def routed_block(rng, own, number, rows, amount, top, reach, skew):
    order = jax.random.permutation(rng, amount)
    crowded, common = portions_of(amount, rows * top, reach, skew, True), portions_of(amount, rows * top, reach, skew, False)
    places = jnp.arange(amount)

    def named(lengths, turn):
        used = int((lengths > 0).sum())
        fixed = max(1, used // 4)
        passed = fixed + (places - fixed + turn * (used - fixed)) % max(1, amount - fixed)
        return jnp.zeros((amount,), jnp.int32).at[order[jnp.where(places < fixed, places, passed)]].set(jnp.asarray(lengths, jnp.int32))

    lengths = jnp.where(number % 4 == 0, named(crowded, number // 4), named(common, number - number // 4 - 1))
    mixed = jax.random.permutation(jax.random.fold_in(own, 3), amount)
    source_of, receiver = mixed[0:amount // 2 * 2:2], mixed[1:amount // 2 * 2:2]
    slack = jnp.minimum(lengths[source_of] - 1, reach - lengths[receiver]) // 2
    slack = jnp.where((source_of == order[0]) | (receiver == order[0]) | (lengths[receiver] == 0), 0, jnp.maximum(slack, 0))
    passed = jax.random.randint(jax.random.fold_in(own, 4), (amount // 2,), 0, 1 << 20) % (slack + 1)
    lengths = lengths.at[source_of].add(-passed).at[receiver].add(passed)
    members = jnp.searchsorted(jnp.cumsum(lengths), jnp.arange(rows * top), side="right").astype(jnp.int32)
    grid = members.reshape(top, rows).T
    grid = grid[jax.random.permutation(jax.random.fold_in(own, 1), rows)]
    turn = jax.random.randint(jax.random.fold_in(own, 2), (rows, 1), 0, top)
    return jnp.take_along_axis(grid, (jnp.arange(top)[None, :] + turn) % top, axis=1)


def portions_of(count, total, limit, skew, full):
    weights = [(1 << 20) // math.isqrt(rank ** skew) + 1 for rank in range(1, count + 1)]
    largest = limit if full else min(limit, max(-(-total // count), total * weights[0] // sum(weights)))
    least = 1 if total - largest >= count - 1 else 0
    counts, surplus = [largest] + [least] * (count - 1), total - largest - least * (count - 1)
    while surplus > 0:
        movable = [i for i in range(1, count) if counts[i] < largest] or [i for i in range(1, count) if counts[i] < limit]
        whole, budget = sum([weights[i] for i in movable]), surplus
        for i in movable:
            addition = min(limit - counts[i], max(1, budget * weights[i] // whole), surplus)
            counts[i] = counts[i] + addition
            surplus = surplus - addition
    return np.array(counts)


def scatter_about(key, dims, scale, most, cuts=(), kind=jnp.bfloat16):
    entries = jax.random.normal(key, dims, jnp.float32) * scale
    if len(cuts) > 0:
        entries = levels(key, dims, cuts, -0.22, 0.18) * entries
    return jnp.clip(entries, min=-most, max=most).astype(kind)


def setup_inputs(seed: int = 0, part: int = 0) -> dict:
    keys = jax.random.split(jax.random.key(seed), 27)
    own_keys = jax.random.split(jax.random.fold_in(keys[26], part), 27)
    layer_input = scatter_about(own_keys[0], (SEQS, D), 1.0, 6.0, ((0, 64),))
    ssm_state = scatter_about(own_keys[1], (2, SEQS, GROUPS, STATE), 0.5, 4.0, ((1, 64), (2, 2)), jnp.float32)
    w_input = scatter_about(keys[2], (D, S5_WIDTH), D ** -0.5, 0.125, ((1, 2),))
    decay_rate = jnp.clip(jnp.exp(math.log(2.0) - 3.6888794 * jax.random.uniform(keys[3], (GROUPS, STATE), jnp.float32) ** levels(keys[3], (GROUPS, STATE), ((0, 2),), -0.2, 0.2)), 0.05, 2.0)
    frequency = jnp.clip(20.0 * jax.random.uniform(keys[4], (GROUPS, STATE), jnp.float32) ** levels(keys[4], (GROUPS, STATE), ((0, 2),), -0.2, 0.2), 0.0, 20.0)
    step_log = jnp.clip(-2.3 + 2.3 * jax.random.uniform(keys[5], (GROUPS,), jnp.float32) ** levels(keys[5], (GROUPS,), ((0, 2),), -0.2, 0.2), -2.3, 0.0)
    input_map = scatter_about(keys[6], (2, GROUPS, STATE, GROUP), (2 * GROUP) ** -0.5, 1.0, ((1, 2),), jnp.float32)
    output_map = scatter_about(keys[7], (2, GROUPS, GROUP, STATE), STATE ** -0.5, 0.75, ((1, 2),), jnp.float32)
    skip_gain = scatter_about(keys[8], (GROUPS, GROUP), 0.5, 3.0, ((0, 2),), jnp.float32)
    glu_weight = scatter_about(keys[9], (S5_WIDTH, S5_WIDTH), S5_WIDTH ** -0.5, 0.25)
    mix_out = scatter_about(keys[10], (S5_WIDTH, D), (S5_WIDTH // 8) ** -0.5, 0.75)
    norm_gain = draw_norm_gain(jax.random.fold_in(keys[26], 71), part)
    norm_shift = scatter_about(keys[12], (D,), 0.3, 2.0, (), jnp.float32)
    route_ids_keys = jax.random.split(jax.random.fold_in(own_keys[13], 1), SEQS // SEQ_DEV)
    route_ids_turns = jax.random.permutation(jax.random.fold_in(own_keys[13], 3), SEQS // SEQ_DEV)
    route_ids = jax.vmap(lambda own, number: routed_block(jax.random.fold_in(own_keys[13], 2), own, number, SEQ_DEV, EXPERTS, TOP_K, CAP, 2))(route_ids_keys, route_ids_turns).reshape((SEQS, TOP_K))
    route_weights = jnp.clip(jnp.exp(math.log(1.0) - 2.3025851 * jax.random.uniform(own_keys[14], (SEQS, TOP_K), jnp.float32) ** levels(own_keys[14], (SEQS, TOP_K), ((0, 64),), -0.2, 0.2)), 0.1, 1.0)
    gate_expert = scatter_about(keys[15], (EXPERTS, D, EFF), D ** -0.5, 0.125, ((0, 64), (2, 2)))
    up_expert = scatter_about(keys[16], (EXPERTS, D, EFF), D ** -0.5, 0.125, ((0, 64), (2, 2)))
    down_expert = scatter_about(keys[17], (EXPERTS, EFF, D), EFF ** -0.5, 0.25, ((0, 64), (1, 2)))
    gate_shared = scatter_about(keys[18], (D, EFF), D ** -0.5, 0.125, ((1, 2),))
    up_shared = scatter_about(keys[19], (D, EFF), D ** -0.5, 0.125, ((1, 2),))
    down_shared = scatter_about(keys[20], (EFF, D), EFF ** -0.5, 0.25, ((0, 2),))
    dense_in = scatter_about(keys[21], (DENSE, D), D ** -0.5, 0.125, ((0, 64),))
    dense_out = scatter_about(keys[22], (DENSE, D), DENSE ** -0.5, 0.1875, ((0, 64), (1, 2)))
    branch_gate = scatter_about(keys[23], (D,), D ** -0.5, 0.125)
    final_gain = jnp.clip(1.0 + 0.18 * jax.random.normal(keys[24], (D,), jnp.float32), 0.1, 1.9)
    final_shift = scatter_about(keys[25], (D,), 0.3, 2.0, ((0, 2),), jnp.float32)
    return dict(layer_input=layer_input, ssm_state=ssm_state, w_input=w_input, decay_rate=decay_rate, frequency=frequency, step_log=step_log, input_map=input_map, output_map=output_map, skip_gain=skip_gain, glu_weight=glu_weight, mix_out=mix_out, norm_gain=norm_gain, norm_shift=norm_shift, route_ids=route_ids, route_weights=route_weights, gate_expert=gate_expert, up_expert=up_expert, down_expert=down_expert, gate_shared=gate_shared, up_shared=up_shared, down_shared=down_shared, dense_in=dense_in, dense_out=dense_out, branch_gate=branch_gate, final_gain=final_gain, final_shift=final_shift)


residual_alpha = 1.681792830507429
route_scale = 2.5
norm_eps = 1e-05
highest = lax.Precision.HIGHEST

def state_update(inputs, ssm_state, decay_rate, frequency, step_log, input_map, output_map, skip_gain):
    step_size = jnp.exp(step_log)[:, None]
    magnitude = jnp.exp(-decay_rate * step_size)
    rotation = frequency * step_size
    decay_re = magnitude * jnp.cos(rotation)
    decay_im = magnitude * jnp.sin(rotation)
    eigen_re = -decay_rate
    denominator = eigen_re * eigen_re + frequency * frequency
    factor_re = ((decay_re - 1.0) * eigen_re + decay_im * frequency) / denominator
    factor_im = (decay_im * eigen_re - (decay_re - 1.0) * frequency) / denominator
    drive_re = factor_re[..., None] * input_map[0] - factor_im[..., None] * input_map[1]
    drive_im = factor_re[..., None] * input_map[1] + factor_im[..., None] * input_map[0]
    pushed_re = jnp.einsum('gpm,tgm->tgp', drive_re, inputs, precision=highest)
    pushed_im = jnp.einsum('gpm,tgm->tgp', drive_im, inputs, precision=highest)
    new_re = decay_re * ssm_state[0] - decay_im * ssm_state[1] + pushed_re
    new_im = decay_re * ssm_state[1] + decay_im * ssm_state[0] + pushed_im
    response = jnp.einsum('gmp,tgp->tgm', output_map[0], new_re, precision=highest) - jnp.einsum('gmp,tgp->tgm', output_map[1], new_im, precision=highest) + skip_gain * inputs
    return (response, jnp.stack([new_re, new_im]))

def layer_norm_rows(values, gain, shift):
    mean = lax.optimization_barrier(jnp.mean(values, axis=1, keepdims=True))
    variance = lax.optimization_barrier(jnp.mean(jnp.square(values - mean), axis=1, keepdims=True))
    return (values - mean) * lax.rsqrt(variance + norm_eps) * gain + shift

def blockwise_down(hidden, down_weight):
    width = hidden.shape[1] // N_TP
    summed = jnp.zeros((hidden.shape[0], down_weight.shape[1]), jnp.float32)
    for portion in range(N_TP):
        part = jnp.dot(hidden[:, portion * width:(portion + 1) * width], down_weight[portion * width:(portion + 1) * width], preferred_element_type=jnp.float32)
        rounded = lax.optimization_barrier(part.astype(jnp.bfloat16))
        summed = summed + rounded.astype(jnp.float32)
    return summed.astype(jnp.bfloat16)

def swiglu_rows(rows, gate_weight, up_weight, down_weight):
    gate_part = jnp.dot(rows, gate_weight, preferred_element_type=jnp.float32)
    up_part = jnp.dot(rows, up_weight, preferred_element_type=jnp.float32)
    hidden = (jax.nn.silu(gate_part) * up_part).astype(jnp.bfloat16)
    return blockwise_down(hidden, down_weight)

def reference(layer_input, ssm_state, w_input, decay_rate, frequency, step_log, input_map, output_map, skip_gain, glu_weight, mix_out, norm_gain, norm_shift, route_ids, route_weights, gate_expert, up_expert, down_expert, gate_shared, up_shared, down_shared, dense_in, dense_out, branch_gate, final_gain, final_shift):
    projected = jnp.dot(layer_input, w_input, preferred_element_type=jnp.float32).astype(jnp.bfloat16)
    inputs = projected.astype(jnp.float32).reshape(SEQS, GROUPS, GROUP)
    response, new_state = state_update(inputs, ssm_state, decay_rate, frequency, step_log, input_map, output_map, skip_gain)
    activated = jax.nn.gelu(response.reshape(SEQS, S5_WIDTH)).astype(jnp.bfloat16)
    glu_out = (activated.astype(jnp.float32) * jax.nn.sigmoid(jnp.dot(activated, glu_weight, preferred_element_type=jnp.float32))).astype(jnp.bfloat16)
    mixed = jnp.dot(glu_out, mix_out, preferred_element_type=jnp.float32).astype(jnp.bfloat16)
    normed = layer_norm_rows(residual_alpha * layer_input.astype(jnp.float32) + mixed.astype(jnp.float32), norm_gain, norm_shift).astype(jnp.bfloat16)
    weights = route_weights / lax.optimization_barrier(jnp.sum(route_weights, axis=1, keepdims=True)) * route_scale
    choices_dev = SEQ_DEV * TOP_K
    block_ids = route_ids.reshape(N_EP, choices_dev)
    hits = (block_ids[..., None] == jnp.arange(EXPERTS, dtype=jnp.int32)).astype(jnp.int32)
    ranks = lax.optimization_barrier(jnp.sum((jnp.cumsum(hits, axis=1) - hits) * hits, axis=2)).astype(jnp.int32)
    sources = jnp.broadcast_to(jnp.arange(N_EP, dtype=jnp.int32)[:, None], (N_EP, choices_dev))
    repeated = jnp.repeat(normed.reshape(N_EP, SEQ_DEV, D), TOP_K, axis=1)
    buffer = jnp.zeros((N_EP, EXPERTS, CAP, D), jnp.bfloat16).at[sources, block_ids, ranks].set(repeated)
    per_expert = jnp.moveaxis(buffer, 1, 0)

    def run_expert(packed):
        slot_rows, gate_weight, up_weight, down_weight = packed
        result = swiglu_rows(slot_rows.reshape(N_EP * CAP, D), gate_weight, up_weight, down_weight)
        return result.reshape(N_EP, CAP, D)
    results = lax.map(run_expert, (per_expert, gate_expert, up_expert, down_expert))
    picked = results[block_ids, sources, ranks].astype(jnp.float32).reshape(SEQS, TOP_K, D)
    routed = lax.optimization_barrier(jnp.sum(picked * weights[:, :, None], axis=1))
    shared = swiglu_rows(normed, gate_shared, up_shared, down_shared)
    dense_hidden = jax.nn.gelu(jnp.dot(normed, dense_in.T, preferred_element_type=jnp.float32)).astype(jnp.bfloat16)
    dense = jnp.dot(dense_hidden, dense_out, preferred_element_type=jnp.float32)
    branch = jax.nn.sigmoid(jnp.dot(normed, branch_gate, preferred_element_type=jnp.float32))
    total = residual_alpha * normed.astype(jnp.float32) + routed + shared.astype(jnp.float32) + branch[:, None] * dense
    mean = lax.optimization_barrier(jnp.mean(total, axis=1, keepdims=True))
    variance = lax.optimization_barrier(jnp.mean(total * total, axis=1, keepdims=True)) - mean * mean
    layer_output = ((total - mean) * lax.rsqrt(variance + norm_eps) * final_gain + final_shift).astype(jnp.bfloat16)
    return (layer_output, new_state)
```

```python
import functools
import math

import jax
import jax.numpy as jnp
from jax import lax
from jax.experimental import pallas as pl
from jax.experimental.pallas import tpu as pltpu
from jax.sharding import PartitionSpec as P

residual_alpha = 1.681792830507429
route_scale = 2.5
norm_eps = 1e-05
highest = lax.Precision.HIGHEST
MESH = pl.DeviceIdType.MESH
f32 = jnp.float32
bf16 = jnp.bfloat16
CHUNKS = 2


def state_update(
    inputs, ssm_state, decay_rate, frequency, step_log, input_map, output_map, skip_gain
):
    step_size = jnp.exp(step_log)[:, None]
    magnitude = jnp.exp(-decay_rate * step_size)
    rotation = frequency * step_size
    decay_re = magnitude * jnp.cos(rotation)
    decay_im = magnitude * jnp.sin(rotation)
    eigen_re = -decay_rate
    denominator = eigen_re * eigen_re + frequency * frequency
    factor_re = ((decay_re - 1.0) * eigen_re + decay_im * frequency) / denominator
    factor_im = (decay_im * eigen_re - (decay_re - 1.0) * frequency) / denominator
    drive_re = factor_re[..., None] * input_map[0] - factor_im[..., None] * input_map[1]
    drive_im = factor_re[..., None] * input_map[1] + factor_im[..., None] * input_map[0]
    pushed_re = jnp.einsum("gpm,tgm->tgp", drive_re, inputs, precision=highest)
    pushed_im = jnp.einsum("gpm,tgm->tgp", drive_im, inputs, precision=highest)
    new_re = decay_re * ssm_state[0] - decay_im * ssm_state[1] + pushed_re
    new_im = decay_re * ssm_state[1] + decay_im * ssm_state[0] + pushed_im
    response = (
        jnp.einsum("gmp,tgp->tgm", output_map[0], new_re, precision=highest)
        - jnp.einsum("gmp,tgp->tgm", output_map[1], new_im, precision=highest)
        + skip_gain * inputs
    )
    return (response, jnp.stack([new_re, new_im]))


def dot(a, b):
    return jnp.dot(a, b, preferred_element_type=f32)


def dot_t(a, b):
    return lax.dot_general(a, b, (((1,), (1,)), ((), ())), preferred_element_type=f32)


def iota(shape, dim):
    return lax.broadcasted_iota(jnp.int32, shape, dim).astype(f32)


def layer_kernel(
    side,
    cap,
    experts,
    act_ref,
    x_ref,
    ids_ref,
    rw_ref,
    gain_ref,
    shift_ref,
    din_ref,
    dout_ref,
    bgate_ref,
    fgain_ref,
    fshift_ref,
    glu_hbm,
    mix_hbm,
    ge_hbm,
    ue_hbm,
    de_hbm,
    gs_hbm,
    us_hbm,
    ds_hbm,
    out_ref,
    glu_v,
    mix_v,
    ge_v,
    ue_v,
    de_v,
    gs_v,
    us_v,
    ds_v,
    act_all,
    meta,
    din_all,
    dout_all,
    own_all,
    oth_all,
    x_send,
    x_recv,
    x_oth,
    y_send,
    y_oth,
    r_send,
    r_recv,
    s_send,
    s_recv,
    sh_send,
    sh_recv,
    st_send,
    st_recv,
    pick_v,
    mix_w,
    dense_v,
    load_sem,
    send_sem,
    recv_sem,
    tsend_sem,
    trecv_sem,
):
    rows, width = x_ref.shape
    half = width // 2
    chunks = own_all.shape[0]
    piece = half // chunks
    line_rows = side * rows
    slots = side * cap
    every = side * slots
    top_k = ids_ref.shape[1]
    core = lax.axis_index("tp")
    chip = lax.axis_index("ep")
    row, col = lax.div(chip, side), lax.rem(chip, side)
    p = (1 - core) * col + core * row
    q = (1 - core) * row + core * col

    def chip_at(pp, qq):
        return (1 - core) * (qq * side + pp) + core * (pp * side + qq)

    def line_peer(d):
        pp = lax.rem(p + d, side)
        return pp, {"ep": chip_at(pp, q), "tp": core}

    def cross_peer(d):
        qq = lax.rem(q + d, side)
        return qq, {"ep": chip_at(p, qq), "tp": core}

    partner = {"ep": chip, "tp": 1 - core}
    order = sorted(range(1, side), key=lambda d: -min(d, side - d))

    META, DIN, DOUT, OTH, OWN = 0, 1, 2, 3, 4
    XS, RS, SS = OWN + chunks, OWN + 2 * chunks, OWN + 3 * chunks

    def to_peer(kind, src, dst, place, device):
        me = q if kind in (DIN, DOUT) or XS <= kind < SS else p
        return pltpu.make_async_remote_copy(
            src_ref=src,
            dst_ref=dst,
            send_sem=send_sem.at[kind, place],
            recv_sem=recv_sem.at[kind, me],
            device_id=device,
            device_id_type=MESH,
        )

    def arrived(kind, dst, place):
        pltpu.make_async_remote_copy(
            src_ref=dst,
            dst_ref=dst,
            send_sem=send_sem.at[kind, place],
            recv_sem=recv_sem.at[kind, place],
            device_id=partner,
            device_id_type=MESH,
        ).wait_recv()

    def to_partner(kind, src, dst):
        return pltpu.make_async_remote_copy(
            src_ref=src,
            dst_ref=dst,
            send_sem=tsend_sem.at[kind],
            recv_sem=trecv_sem.at[kind],
            device_id=partner,
            device_id_type=MESH,
        )

    loads = [
        pltpu.make_async_copy(s, d, load_sem.at[i])
        for i, (s, d) in enumerate(
            [
                (glu_hbm, glu_v),
                (mix_hbm, mix_v),
                (gs_hbm, gs_v),
                (us_hbm, us_v),
                (ds_hbm, ds_v),
                (ge_hbm, ge_v),
                (ue_hbm, ue_v),
                (de_hbm, de_v),
            ]
        )
    ]
    for load in loads:
        load.start()

    barrier = pltpu.get_barrier_semaphore()
    pl.semaphore_signal(barrier, inc=1, device_id=partner, device_id_type=MESH)
    for d in range(1, side):
        for _, device in (line_peer(d), cross_peer(d)):
            pl.semaphore_signal(barrier, inc=1, device_id=device, device_id_type=MESH)
    pl.semaphore_wait(barrier, 2 * side - 1)

    sends = []

    def go(copy):
        copy.start()
        sends.append(copy)
        return copy

    act_copy = go(to_partner(0, act_ref, act_all.at[core]))
    act_all[core] = act_ref[...]

    lanes = meta.shape[3]
    ids, scores = ids_ref[...].astype(f32), rw_ref[...]
    scores = scores / jnp.sum(scores, axis=1, keepdims=True) * route_scale
    lane = iota((rows, lanes), 1)
    hits = jnp.zeros((rows, lanes), f32)
    share = jnp.zeros((rows, lanes), f32)
    for k in range(top_k):
        here = jnp.where(lane == ids[:, k : k + 1], 1.0, 0.0)
        hits += here
        share += here * scores[:, k : k + 1]
    earlier = jnp.where(iota((rows, rows), 1) < iota((rows, rows), 0), 1.0, 0.0)
    ranks = dot(earlier.astype(bf16), hits.astype(bf16))
    meta[p, 0] = jnp.where(hits > 0.5, ranks, -1.0).astype(bf16)
    meta[p, 1] = share.astype(bf16)
    din_all[q] = din_ref[...]
    dout_all[q] = dout_ref[...]
    for d in order:
        place, device = line_peer(d)
        go(to_peer(META, meta.at[p], meta.at[p], place, device))
    for d in order:
        place, device = cross_peer(d)
        go(to_peer(DIN, din_ref, din_all.at[q], place, device))
        go(to_peer(DOUT, dout_ref, dout_all.at[q], place, device))

    loads[0].wait()
    loads[1].wait()
    act_copy.wait_recv()
    channels = act_ref.shape[1]
    a0, a1 = act_all[0], act_all[1]
    gate = dot(a0, glu_v[:channels]) + dot(a1, glu_v[channels:])
    g0 = (a0.astype(f32) * jax.nn.sigmoid(gate[:, :channels])).astype(bf16)
    g1 = (a1.astype(f32) * jax.nn.sigmoid(gate[:, channels:])).astype(bf16)
    mixed = (dot(g0, mix_v[:channels]) + dot(g1, mix_v[channels:])).astype(bf16)
    values = residual_alpha * x_ref[...].astype(f32) + mixed.astype(f32)
    mean = jnp.mean(values, axis=1, keepdims=True)
    centred = values - mean
    variance = jnp.mean(centred * centred, axis=1, keepdims=True)
    normed = (centred * lax.rsqrt(variance + norm_eps) * gain_ref[...] + shift_ref[...]).astype(
        bf16
    )
    left, right = normed[:, :half], normed[:, half:]
    first = core == 0
    own = jnp.where(first, left, right)
    oth = jnp.where(first, right, left)
    for i in range(chunks):
        own_all[i, p] = own[:, i * piece : (i + 1) * piece]
    oth_all[p] = oth
    for i in range(chunks):
        for d in order:
            place, device = line_peer(d)
            go(to_peer(OWN + i, own_all.at[i, p], own_all.at[i, p], place, device))
    for d in order:
        place, device = line_peer(d)
        go(to_peer(OTH, oth_all.at[p], oth_all.at[p], place, device))

    for d in order:
        place, _ = line_peer(d)
        arrived(META, meta.at[place], place)
    lane = iota((1, every), 1)
    at_q = jnp.floor((lane + 0.5) / slots)
    at_p = jnp.floor((lane - at_q * slots + 0.5) / cap)
    at_rank = lane - at_q * slots - at_p * cap
    pf, cf = p.astype(f32), core.astype(f32)
    expert = (1.0 - cf) * (at_q * side + pf) + cf * (pf * side + at_q)
    spread = jnp.where(iota((lanes, every), 0) == expert, 1.0, 0.0).astype(bf16)
    codes = dot(meta[:, 0].reshape(line_rows, lanes), spread)
    shares = dot(meta[:, 1].reshape(line_rows, lanes), spread)
    block = jnp.floor((iota((line_rows, 1), 0) + 0.5) / rows)
    chosen = jnp.where((codes == at_rank) & (block == at_p), 1.0, 0.0)
    mix_w[...] = (chosen * shares).astype(bf16)
    pick_v[...] = chosen.T.astype(bf16)

    for load in loads[2:5]:
        load.wait()
    hidden = (jax.nn.silu(dot(normed, gs_v[...])) * dot(normed, us_v[...])).astype(bf16)
    base = core * half
    other = (1 - core) * half
    sh_send[...] = dot(hidden, ds_v[:, pl.ds(pl.multiple_of(other, 128), half)]).astype(bf16)
    shared_copy = go(to_partner(1, sh_send, sh_recv))
    shared_own = dot(hidden, ds_v[:, pl.ds(pl.multiple_of(base, 128), half)]).astype(bf16)

    for i in range(chunks):
        for d in order:
            place, _ = line_peer(d)
            arrived(OWN + i, own_all.at[i, place], place)
        picked = dot(pick_v[...], own_all[i].reshape(line_rows, piece)).astype(bf16)
        x_send[i] = picked.reshape(side, slots, piece)
        for d in order:
            place, device = cross_peer(d)
            go(to_peer(XS + i, x_send.at[i, place], x_recv.at[i, q], place, device))
        x_recv[i, q] = x_send[i, q]

    for d in order:
        place, _ = line_peer(d)
        arrived(OTH, oth_all.at[place], place)
    for d in order:
        place, _ = cross_peer(d)
        arrived(DIN, din_all.at[place], place)
        arrived(DOUT, dout_all.at[place], place)
    units = side * din_ref.shape[0]
    din = din_all[...].reshape(units, width)
    din_left, din_right = din[:, :half], din[:, half:]
    din_own = jnp.where(first, din_left, din_right)
    din_oth = jnp.where(first, din_right, din_left)
    bgate = jnp.broadcast_to(bgate_ref[...], (8, width))
    b_own = jnp.where(first, bgate[:, :half], bgate[:, half:])
    b_oth = jnp.where(first, bgate[:, half:], bgate[:, :half])
    oth_tok = oth_all[...].reshape(line_rows, half)
    before = dot_t(oth_tok, din_oth)
    gate = dot_t(oth_tok, b_oth)
    for i in range(chunks):
        tok = own_all[i].reshape(line_rows, piece)
        before += dot_t(tok, din_own[:, i * piece : (i + 1) * piece])
        gate += dot_t(tok, b_own[:, i * piece : (i + 1) * piece])
    dense_hidden = jax.nn.gelu(before).astype(bf16)
    branch = jax.nn.sigmoid(gate[:, :1])
    dense_v[...] = branch * dot(dense_hidden, dout_all[...].reshape(units, half))

    r0, r1 = iota((every, 1), 0), iota((1, every), 1)
    a = jnp.floor((r0 + 0.5) / slots)
    b = jnp.floor((r0 - a * slots + 0.5) / cap)
    swap = jnp.where(r1 == b * slots + a * cap + (r0 - a * slots - b * cap), 1.0, 0.0).astype(bf16)

    for i in range(chunks):
        for d in order:
            place, _ = cross_peer(d)
            arrived(XS + i, x_recv.at[i, place], place)
        go(to_partner(4 + i, x_recv.at[i], x_oth.at[i]))
    for load in loads[5:]:
        load.wait()
    units = ge_v.shape[1]
    gate = jnp.zeros((every, units), f32)
    up = jnp.zeros((every, units), f32)
    for i in range(chunks):
        tok = x_recv[i].reshape(every, piece)
        at = pl.ds(pl.multiple_of(base + i * piece, 128), piece)
        gate += dot(tok, ge_v[at])
        up += dot(tok, ue_v[at])
    for i in range(chunks):
        to_partner(4 + i, x_recv.at[i], x_oth.at[i]).wait_recv()
        tok = dot(swap, x_oth[i].reshape(every, piece)).astype(bf16)
        at = pl.ds(pl.multiple_of(other + i * piece, 128), piece)
        gate += dot(tok, ge_v[at])
        up += dot(tok, ue_v[at])
    hidden = (jax.nn.silu(gate) * up).astype(bf16)
    y_send[...] = dot(hidden, de_v[:, pl.ds(pl.multiple_of(other, 128), half)]).astype(bf16)
    y_copy = go(to_partner(2, y_send, y_oth))
    result = dot(hidden, de_v[:, pl.ds(pl.multiple_of(base, 128), half)])
    y_copy.wait_recv()
    for i in range(chunks):
        at = slice(i * piece, (i + 1) * piece)
        theirs = dot(swap, y_oth[:, at])
        r_send[i] = (result[:, at] + theirs).astype(bf16).reshape(side, slots, piece)
        for d in order:
            place, device = cross_peer(d)
            go(to_peer(RS + i, r_send.at[i, place], r_recv.at[i, q], place, device))
        r_recv[i, q] = r_send[i, q]

    for i in range(chunks):
        for d in order:
            place, _ = cross_peer(d)
            arrived(RS + i, r_recv.at[i, place], place)
        part = dot(mix_w[...], r_recv[i].reshape(every, piece))
        part += dense_v[:, i * piece : (i + 1) * piece]
        s_send[i] = part.astype(bf16).reshape(side, rows, piece)
        for d in order:
            place, device = line_peer(d)
            go(to_peer(SS + i, s_send.at[i, place], s_recv.at[i, p], place, device))
        s_recv[i, p] = s_send[i, p]

    shared_copy.wait_recv()
    shared = (shared_own.astype(f32) + sh_recv[...].astype(f32)).astype(bf16).astype(f32)
    skip = residual_alpha * own.astype(f32) + shared
    totals = []
    for i in range(chunks):
        for d in order:
            place, _ = line_peer(d)
            arrived(SS + i, s_recv.at[i, place], place)
        total = skip[:, i * piece : (i + 1) * piece]
        for j in range(side):
            total += s_recv[i, j].astype(f32)
        totals.append(total)
    row_sum = sum(jnp.sum(t, axis=1, keepdims=True) for t in totals)
    row_squares = sum(jnp.sum(t * t, axis=1, keepdims=True) for t in totals)
    st_send[...] = jnp.where(iota(st_send.shape, 1) < 0.5, row_sum, row_squares)
    st_copy = go(to_partner(3, st_send, st_recv))
    st_copy.wait_recv()
    mean = (row_sum + st_recv[:, 0:1]) / width
    variance = (row_squares + st_recv[:, 1:2]) / width - mean * mean
    scale = lax.rsqrt(variance + norm_eps)
    for i in range(chunks):
        at = slice(i * piece, (i + 1) * piece)
        out_ref[:, at] = ((totals[i] - mean) * scale * fgain_ref[:, at] + fshift_ref[:, at]).astype(
            bf16
        )
    for copy in sends:
        copy.wait_send()


def layer(side, cap, experts, vmem_args, hbm_args):
    rows, width = vmem_args[1].shape
    channels = vmem_args[0].shape[1]
    half = width // 2
    chunks = CHUNKS
    piece = half // chunks
    slots = side * cap
    every = side * slots
    lanes = -(-experts // 128) * 128
    din, dout = vmem_args[6], vmem_args[7]
    kinds = 4 + 4 * chunks
    V = pltpu.VMEM
    return pl.pallas_call(
        functools.partial(layer_kernel, side, cap, experts),
        out_shape=jax.ShapeDtypeStruct((rows, half), bf16),
        in_specs=[pl.BlockSpec(memory_space=pltpu.VMEM)] * len(vmem_args)
        + [pl.BlockSpec(memory_space=pl.ANY)] * len(hbm_args),
        out_specs=pl.BlockSpec(memory_space=pltpu.VMEM),
        scratch_shapes=[V(a.shape, bf16) for a in hbm_args]
        + [
            V((2, rows, channels), bf16),
            V((side, 2, rows, lanes), bf16),
            V((side, *din.shape), bf16),
            V((side, *dout.shape), bf16),
            V((chunks, side, rows, piece), bf16),
            V((side, rows, half), bf16),
            V((chunks, side, slots, piece), bf16),
            V((chunks, side, slots, piece), bf16),
            V((chunks, side, slots, piece), bf16),
            V((every, half), bf16),
            V((every, half), bf16),
            V((chunks, side, slots, piece), bf16),
            V((chunks, side, slots, piece), bf16),
            V((chunks, side, rows, piece), bf16),
            V((chunks, side, rows, piece), bf16),
            V((rows, half), bf16),
            V((rows, half), bf16),
            V((rows, 128), f32),
            V((rows, 128), f32),
            V((every, side * rows), bf16),
            V((side * rows, every), bf16),
            V((side * rows, half), f32),
            pltpu.SemaphoreType.DMA((len(hbm_args),)),
            pltpu.SemaphoreType.DMA((kinds, side)),
            pltpu.SemaphoreType.DMA((kinds, side)),
            pltpu.SemaphoreType.DMA((4 + chunks,)),
            pltpu.SemaphoreType.DMA((4 + chunks,)),
        ],
        compiler_params=pltpu.CompilerParams(
            collective_id=0, has_side_effects=True, vmem_limit_bytes=48 * 1024 * 1024
        ),
        name="layer",
    )(*vmem_args, *hbm_args)


def body(
    layer_input,
    ssm_state,
    w_input,
    decay_rate,
    frequency,
    step_log,
    input_map,
    output_map,
    skip_gain,
    glu_weight,
    mix_out,
    norm_gain,
    norm_shift,
    route_ids,
    route_weights,
    gate_expert,
    up_expert,
    down_expert,
    gate_shared,
    up_shared,
    down_shared,
    dense_in,
    dense_out,
    branch_gate,
    final_gain,
    final_shift,
):
    count_ep = lax.axis_size("ep")
    count_tp = lax.axis_size("tp")
    seq_rows, width = layer_input.shape
    local_groups, channels = skip_gain.shape
    projected = jnp.dot(layer_input, w_input, preferred_element_type=f32).astype(bf16)
    inputs = projected.astype(f32).reshape(seq_rows, local_groups, channels)
    response, new_state = state_update(
        inputs, ssm_state, decay_rate, frequency, step_log, input_map, output_map, skip_gain
    )
    activated = jax.nn.gelu(response.reshape(seq_rows, local_groups * channels)).astype(bf16)
    top_k = route_ids.shape[1]
    experts = gate_expert.shape[0] * count_ep
    cap = count_tp * max(1, min(seq_rows // count_tp, seq_rows * top_k // experts))
    side = math.isqrt(count_ep)
    layer_output = layer(
        side,
        cap,
        experts,
        [
            activated,
            layer_input,
            route_ids,
            route_weights,
            norm_gain[None],
            norm_shift[None],
            dense_in,
            dense_out,
            branch_gate[None],
            final_gain[None],
            final_shift[None],
        ],
        [
            glu_weight,
            mix_out,
            gate_expert[0],
            up_expert[0],
            down_expert[0],
            gate_shared,
            up_shared,
            down_shared,
        ],
    )
    return (layer_output, new_state)


def solution(mesh):
    placed = (
        P(("grp", "ep"), None),
        P(None, ("grp", "ep"), "tp", None),
        P(None, "tp"),
        P("tp", None),
        P("tp", None),
        P("tp"),
        P(None, "tp", None, None),
        P(None, "tp", None, None),
        P("tp", None),
        P(),
        P(),
        P(),
        P(),
        P(("grp", "ep"), None),
        P(("grp", "ep"), None),
        P("ep", None, "tp"),
        P("ep", None, "tp"),
        P("ep", "tp", None),
        P(None, "tp"),
        P(None, "tp"),
        P("tp", None),
        P("ep", None),
        P("ep", "tp"),
        P(),
        P("tp"),
        P("tp"),
    )
    return jax.shard_map(
        body,
        mesh=mesh,
        in_specs=placed,
        out_specs=(P(("grp", "ep"), "tp"), P(None, ("grp", "ep"), "tp", None)),
        check_vma=False,
    )
```

```python
import functools
import math

import jax
import jax.numpy as jnp
from jax import lax
from jax.experimental import pallas as pl
from jax.experimental.pallas import tpu as pltpu
from jax.sharding import PartitionSpec as P

residual_alpha = 1.681792830507429
route_scale = 2.5
norm_eps = 1e-05
highest = lax.Precision.HIGHEST
MESH = pl.DeviceIdType.MESH
f32 = jnp.float32
bf16 = jnp.bfloat16
CHUNKS = 2
VMEM_BYTES = 64 * 1024 * 1024 - 1024 * 1024


def dot(a, b):
    return jnp.dot(a, b, preferred_element_type=f32)


def dot_t(a, b):
    return lax.dot_general(a, b, (((1,), (1,)), ((), ())), preferred_element_type=f32)


def iota(shape, dim):
    return lax.broadcasted_iota(jnp.int32, shape, dim).astype(f32)


def halves(a):
    high = a.astype(bf16)
    return high, (a - high.astype(f32)).astype(bf16)


def layer_kernel(side, cap, names, *refs):
    count = len(names)
    hbm = refs[:count]
    out_ref, new_ref = refs[count : count + 2]
    local = dict(zip(names, refs[count + 2 :]))
    rest = refs[2 * count + 2 :]
    layer_steps(side, cap, names, hbm, local, out_ref, new_ref, *rest)


def layer_steps(
    side,
    cap,
    names,
    hbm,
    local,
    out_ref,
    new_ref,
    drive_v,
    omap_v,
    act_send,
    act_all,
    meta,
    din_all,
    dout_all,
    own_all,
    oth_all,
    x_send,
    x_recv,
    x_oth,
    y_send,
    y_oth,
    r_send,
    r_recv,
    s_send,
    s_recv,
    sh_send,
    sh_recv,
    st_send,
    st_recv,
    pick_v,
    mix_w,
    dense_v,
    load_sem,
    send_sem,
    recv_sem,
    tsend_sem,
    trecv_sem,
):
    x_ref, din_ref, dout_ref = local["x"], local["din"], local["dout"]
    rows, width = x_ref.shape
    half = width // 2
    chunks = own_all.shape[0]
    piece = half // chunks
    line_rows = side * rows
    slots = side * cap
    every = side * slots
    core = lax.axis_index("tp")
    chip = lax.axis_index("ep")
    row, col = lax.div(chip, side), lax.rem(chip, side)
    p = (1 - core) * col + core * row
    q = (1 - core) * row + core * col

    def chip_at(pp, qq):
        return (1 - core) * (qq * side + pp) + core * (pp * side + qq)

    def line_peer(d):
        pp = lax.rem(p + d, side)
        return pp, {"ep": chip_at(pp, q), "tp": core}

    def cross_peer(d):
        qq = lax.rem(q + d, side)
        return qq, {"ep": chip_at(p, qq), "tp": core}

    partner = {"ep": chip, "tp": 1 - core}
    order = sorted(range(1, side), key=lambda d: -min(d, side - d))

    META, DIN, DOUT, OTH, OWN = 0, 1, 2, 3, 4
    XS, RS, SS = OWN + chunks, OWN + 2 * chunks, OWN + 3 * chunks

    def to_peer(kind, src, dst, place, device):
        me = q if kind in (DIN, DOUT) or XS <= kind < SS else p
        return pltpu.make_async_remote_copy(
            src_ref=src,
            dst_ref=dst,
            send_sem=send_sem.at[kind, place],
            recv_sem=recv_sem.at[kind, me],
            device_id=device,
            device_id_type=MESH,
        )

    def arrived(kind, dst, place):
        pltpu.make_async_remote_copy(
            src_ref=dst,
            dst_ref=dst,
            send_sem=send_sem.at[kind, place],
            recv_sem=recv_sem.at[kind, place],
            device_id=partner,
            device_id_type=MESH,
        ).wait_recv()

    def to_partner(kind, src, dst):
        return pltpu.make_async_remote_copy(
            src_ref=src,
            dst_ref=dst,
            send_sem=tsend_sem.at[kind],
            recv_sem=trecv_sem.at[kind],
            device_id=partner,
            device_id_type=MESH,
        )

    loads = {
        name: pltpu.make_async_copy(src, local[name], load_sem.at[i])
        for i, (name, src) in enumerate(zip(names, hbm))
    }
    for load in loads.values():
        load.start()

    def loaded(*wanted):
        for name in wanted:
            loads[name].wait()

    barrier = pltpu.get_barrier_semaphore()
    pl.semaphore_signal(barrier, inc=1, device_id=partner, device_id_type=MESH)
    for d in range(1, side):
        for _, device in (line_peer(d), cross_peer(d)):
            pl.semaphore_signal(barrier, inc=1, device_id=device, device_id_type=MESH)

    lanes = meta.shape[3]
    loaded("ids", "scores")
    ids, scores = local["ids"][...].astype(f32), local["scores"][...]
    scores = scores / jnp.sum(scores, axis=0, keepdims=True) * route_scale
    eye = iota((rows, rows), 0) == iota((rows, rows), 1)
    lane = iota((rows, lanes), 1)
    hits = jnp.zeros((rows, lanes), f32)
    share = jnp.zeros((rows, lanes), f32)
    for k in range(ids.shape[0]):
        name = jnp.sum(jnp.where(eye, ids[k : k + 1], 0.0), axis=1, keepdims=True)
        score = jnp.sum(jnp.where(eye, scores[k : k + 1], 0.0), axis=1, keepdims=True)
        here = jnp.where(lane == name, 1.0, 0.0)
        hits += here
        share += here * score
    earlier = jnp.where(iota((rows, rows), 1) < iota((rows, rows), 0), 1.0, 0.0)
    ranks = dot(earlier.astype(bf16), hits.astype(bf16))
    meta[p, 0] = jnp.where(hits > 0.5, ranks, -1.0).astype(bf16)
    meta[p, 1] = share.astype(bf16)

    groups, states = local["rate"].shape
    members = local["skip"].shape[1]
    channels = groups * members
    pair = 2 * states
    drive_v[...] = jnp.zeros_like(drive_v)
    omap_v[...] = jnp.zeros_like(omap_v)
    loaded("rate", "freq", "step", "imap", "omap", "skip")
    rate, freq = local["rate"][...], local["freq"][...]
    eye = iota((groups, groups), 0) == iota((groups, groups), 1)
    step = jnp.exp(jnp.sum(jnp.where(eye, local["step"][...], 0.0), axis=1, keepdims=True))
    magnitude = jnp.exp(-rate * step)
    angle = freq * step
    decay_re, decay_im = magnitude * jnp.cos(angle), magnitude * jnp.sin(angle)
    denominator = rate * rate + freq * freq
    factor_re = ((decay_re - 1.0) * -rate + decay_im * freq) / denominator
    factor_im = (decay_im * -rate - (decay_re - 1.0) * freq) / denominator
    same = jnp.concatenate([decay_re, decay_re], axis=1)
    cross = jnp.concatenate([-decay_im, decay_im], axis=1)
    for g in range(groups):
        fr, fi = factor_re[g : g + 1], factor_im[g : g + 1]
        m0, m1 = local["imap"][0, g], local["imap"][1, g]
        drive = jnp.concatenate([fr * m0 - fi * m1, fr * m1 + fi * m0], axis=1)
        out = jnp.concatenate([local["omap"][0, g], -local["omap"][1, g]], axis=1)
        at, lanes_at = slice(g * members, (g + 1) * members), slice(g * pair, (g + 1) * pair)
        drive_v[0, at, lanes_at], drive_v[1, at, lanes_at] = halves(drive)
        omap_v[0, at, lanes_at], omap_v[1, at, lanes_at] = halves(out)
    tile = jnp.where(
        iota((members, channels), 0)
        == iota((members, channels), 1)
        - jnp.floor((iota((members, channels), 1) + 0.5) / members) * members,
        1.0,
        0.0,
    )
    skip = jnp.dot(local["skip"][...], tile, preferred_element_type=f32, precision=highest)
    in_group = jnp.floor((iota((groups, channels), 1) + 0.5) / members) == iota(
        (groups, channels), 0
    )
    skip = jnp.sum(jnp.where(in_group, skip, 0.0), axis=0, keepdims=True)
    loaded("x", "win")
    projected = dot(x_ref[...], local["win"][...]).astype(bf16)
    pushed = dot(projected, drive_v[0]) + dot(projected, drive_v[1])
    loaded("state")
    response = skip * projected.astype(f32)
    highs, lows = [], []
    for g in range(groups):
        old = jnp.concatenate(
            [
                local["state"][pl.ds(g, rows, stride=groups)],
                local["state"][pl.ds(rows * groups + g, rows, stride=groups)],
            ],
            axis=1,
        )
        turned = jnp.concatenate([old[:, states:], old[:, :states]], axis=1)
        new = same[g : g + 1] * old + cross[g : g + 1] * turned
        new += pushed[:, g * pair : (g + 1) * pair]
        new_ref[pl.ds(g, rows, stride=groups)] = new[:, :states]
        new_ref[pl.ds(rows * groups + g, rows, stride=groups)] = new[:, states:]
        high, low = halves(new)
        highs.append(high)
        lows.append(low)
    high, low = jnp.concatenate(highs, axis=1), jnp.concatenate(lows, axis=1)
    response += dot_t(high, omap_v[0]) + dot_t(high, omap_v[1]) + dot_t(low, omap_v[0])
    act_send[...] = jax.nn.gelu(response).astype(bf16)

    pl.semaphore_wait(barrier, 2 * side - 1)
    sends = []

    def go(copy):
        copy.start()
        sends.append(copy)
        return copy

    act_copy = go(to_partner(0, act_send, act_all.at[core]))
    act_all[core] = act_send[...]
    loaded("din", "dout")
    din_all[q] = din_ref[...]
    dout_all[q] = dout_ref[...]
    for d in order:
        place, device = line_peer(d)
        go(to_peer(META, meta.at[p], meta.at[p], place, device))
    for d in order:
        place, device = cross_peer(d)
        go(to_peer(DIN, din_ref, din_all.at[q], place, device))
        go(to_peer(DOUT, dout_ref, dout_all.at[q], place, device))

    loaded("glu", "mix", "gain", "shift")
    glu_v, mix_v = local["glu"], local["mix"]
    act_copy.wait_recv()
    a0, a1 = act_all[0], act_all[1]
    gate = dot(a0, glu_v[:channels]) + dot(a1, glu_v[channels:])
    g0 = (a0.astype(f32) * jax.nn.sigmoid(gate[:, :channels])).astype(bf16)
    g1 = (a1.astype(f32) * jax.nn.sigmoid(gate[:, channels:])).astype(bf16)
    mixed = (dot(g0, mix_v[:channels]) + dot(g1, mix_v[channels:])).astype(bf16)
    values = residual_alpha * x_ref[...].astype(f32) + mixed.astype(f32)
    mean = jnp.mean(values, axis=1, keepdims=True)
    centred = values - mean
    variance = jnp.mean(centred * centred, axis=1, keepdims=True)
    normed = (centred * lax.rsqrt(variance + norm_eps) * local["gain"][...] + local["shift"][...]).astype(
        bf16
    )
    left, right = normed[:, :half], normed[:, half:]
    first = core == 0
    own = jnp.where(first, left, right)
    oth = jnp.where(first, right, left)
    for i in range(chunks):
        own_all[i, p] = own[:, i * piece : (i + 1) * piece]
    oth_all[p] = oth
    for i in range(chunks):
        for d in order:
            place, device = line_peer(d)
            go(to_peer(OWN + i, own_all.at[i, p], own_all.at[i, p], place, device))

    for d in order:
        place, _ = line_peer(d)
        arrived(META, meta.at[place], place)
    lane = iota((1, every), 1)
    at_q = jnp.floor((lane + 0.5) / slots)
    at_p = jnp.floor((lane - at_q * slots + 0.5) / cap)
    at_rank = lane - at_q * slots - at_p * cap
    pf, cf = p.astype(f32), core.astype(f32)
    expert = (1.0 - cf) * (at_q * side + pf) + cf * (pf * side + at_q)
    spread = jnp.where(iota((lanes, every), 0) == expert, 1.0, 0.0).astype(bf16)
    codes = dot(meta[:, 0].reshape(line_rows, lanes), spread)
    shares = dot(meta[:, 1].reshape(line_rows, lanes), spread)
    block = jnp.floor((iota((line_rows, 1), 0) + 0.5) / rows)
    chosen = jnp.where((codes == at_rank) & (block == at_p), 1.0, 0.0)
    mix_w[...] = (chosen * shares).astype(bf16)
    pick_v[...] = chosen.T.astype(bf16)

    loaded("gs", "us", "ds")
    gs_v, us_v, ds_v = local["gs"], local["us"], local["ds"]
    hidden = (jax.nn.silu(dot(normed, gs_v[...])) * dot(normed, us_v[...])).astype(bf16)
    base = core * half
    other = (1 - core) * half
    sh_send[...] = dot(hidden, ds_v[:, pl.ds(pl.multiple_of(other, 128), half)]).astype(bf16)
    shared_copy = go(to_partner(1, sh_send, sh_recv))
    shared_own = dot(hidden, ds_v[:, pl.ds(pl.multiple_of(base, 128), half)]).astype(bf16)

    for i in range(chunks):
        for d in order:
            place, _ = line_peer(d)
            arrived(OWN + i, own_all.at[i, place], place)
        picked = dot(pick_v[...], own_all[i].reshape(line_rows, piece)).astype(bf16)
        x_send[i] = picked.reshape(side, slots, piece)
        for d in order:
            place, device = cross_peer(d)
            go(to_peer(XS + i, x_send.at[i, place], x_recv.at[i, q], place, device))
        x_recv[i, q] = x_send[i, q]

    r0, r1 = iota((every, 1), 0), iota((1, every), 1)
    a = jnp.floor((r0 + 0.5) / slots)
    b = jnp.floor((r0 - a * slots + 0.5) / cap)
    swap = jnp.where(r1 == b * slots + a * cap + (r0 - a * slots - b * cap), 1.0, 0.0).astype(bf16)

    for i in range(chunks):
        for d in order:
            place, _ = cross_peer(d)
            arrived(XS + i, x_recv.at[i, place], place)
        go(to_partner(4 + i, x_recv.at[i], x_oth.at[i]))
    for d in order:
        place, device = line_peer(d)
        go(to_peer(OTH, oth_all.at[p], oth_all.at[p], place, device))
    loaded("ge", "ue", "de")
    ge_v, ue_v, de_v = local["ge"], local["ue"], local["de"]
    units = ge_v.shape[1]
    gate = jnp.zeros((every, units), f32)
    up = jnp.zeros((every, units), f32)
    for i in range(chunks):
        tok = x_recv[i].reshape(every, piece)
        at = pl.ds(pl.multiple_of(base + i * piece, 128), piece)
        gate += dot(tok, ge_v[at])
        up += dot(tok, ue_v[at])
    for i in range(chunks):
        to_partner(4 + i, x_recv.at[i], x_oth.at[i]).wait_recv()
        tok = dot(swap, x_oth[i].reshape(every, piece)).astype(bf16)
        at = pl.ds(pl.multiple_of(other + i * piece, 128), piece)
        gate += dot(tok, ge_v[at])
        up += dot(tok, ue_v[at])
    hidden = (jax.nn.silu(gate) * up).astype(bf16)
    y_send[...] = dot(hidden, de_v[:, pl.ds(pl.multiple_of(other, 128), half)]).astype(bf16)
    y_copy = go(to_partner(2, y_send, y_oth))
    result = dot(hidden, de_v[:, pl.ds(pl.multiple_of(base, 128), half)])
    y_copy.wait_recv()
    for i in range(chunks):
        at = slice(i * piece, (i + 1) * piece)
        theirs = dot(swap, y_oth[:, at])
        r_send[i] = (result[:, at] + theirs).astype(bf16).reshape(side, slots, piece)
        for d in order:
            place, device = cross_peer(d)
            go(to_peer(RS + i, r_send.at[i, place], r_recv.at[i, q], place, device))
        r_recv[i, q] = r_send[i, q]

    for d in order:
        place, _ = line_peer(d)
        arrived(OTH, oth_all.at[place], place)
    for d in order:
        place, _ = cross_peer(d)
        arrived(DIN, din_all.at[place], place)
        arrived(DOUT, dout_all.at[place], place)
    units = side * din_ref.shape[0]
    din = din_all[...].reshape(units, width)
    din_left, din_right = din[:, :half], din[:, half:]
    din_own = jnp.where(first, din_left, din_right)
    din_oth = jnp.where(first, din_right, din_left)
    loaded("bgate")
    bgate = jnp.broadcast_to(local["bgate"][...], (8, width))
    b_own = jnp.where(first, bgate[:, :half], bgate[:, half:])
    b_oth = jnp.where(first, bgate[:, half:], bgate[:, :half])
    oth_tok = oth_all[...].reshape(line_rows, half)
    before = dot_t(oth_tok, din_oth)
    gate = dot_t(oth_tok, b_oth)
    for i in range(chunks):
        tok = own_all[i].reshape(line_rows, piece)
        before += dot_t(tok, din_own[:, i * piece : (i + 1) * piece])
        gate += dot_t(tok, b_own[:, i * piece : (i + 1) * piece])
    dense_hidden = jax.nn.gelu(before).astype(bf16)
    branch = jax.nn.sigmoid(gate[:, :1])
    dense_v[...] = branch * dot(dense_hidden, dout_all[...].reshape(units, half))

    for i in range(chunks):
        for d in order:
            place, _ = cross_peer(d)
            arrived(RS + i, r_recv.at[i, place], place)
        part = dot(mix_w[...], r_recv[i].reshape(every, piece))
        part += dense_v[:, i * piece : (i + 1) * piece]
        s_send[i] = part.astype(bf16).reshape(side, rows, piece)
        for d in order:
            place, device = line_peer(d)
            go(to_peer(SS + i, s_send.at[i, place], s_recv.at[i, p], place, device))
        s_recv[i, p] = s_send[i, p]

    shared_copy.wait_recv()
    shared = (shared_own.astype(f32) + sh_recv[...].astype(f32)).astype(bf16).astype(f32)
    skip = residual_alpha * own.astype(f32) + shared
    totals = []
    for i in range(chunks):
        for d in order:
            place, _ = line_peer(d)
            arrived(SS + i, s_recv.at[i, place], place)
        total = skip[:, i * piece : (i + 1) * piece]
        for j in range(side):
            total += s_recv[i, j].astype(f32)
        totals.append(total)
    loaded("fgain", "fshift")
    row_sum = sum(jnp.sum(t, axis=1, keepdims=True) for t in totals)
    row_squares = sum(jnp.sum(t * t, axis=1, keepdims=True) for t in totals)
    st_send[...] = jnp.where(iota(st_send.shape, 1) < 0.5, row_sum, row_squares)
    st_copy = go(to_partner(3, st_send, st_recv))
    st_copy.wait_recv()
    mean = (row_sum + st_recv[:, 0:1]) / width
    variance = (row_squares + st_recv[:, 1:2]) / width - mean * mean
    scale = lax.rsqrt(variance + norm_eps)
    for i in range(chunks):
        at = slice(i * piece, (i + 1) * piece)
        out_ref[:, at] = ((totals[i] - mean) * scale * local["fgain"][:, at] + local["fshift"][:, at]).astype(
            bf16
        )
    for copy in sends:
        copy.wait_send()


def layer(side, cap, experts, args):
    names = tuple(args)
    rows, width = args["x"].shape
    groups, states = args["rate"].shape
    channels = args["win"].shape[1]
    half = width // 2
    chunks = CHUNKS
    piece = half // chunks
    slots = side * cap
    every = side * slots
    lanes = -(-experts // 128) * 128
    din, dout = args["din"], args["dout"]
    kinds = 4 + 4 * chunks
    V = pltpu.VMEM
    return pl.pallas_call(
        functools.partial(layer_kernel, side, cap, names),
        out_shape=(
            jax.ShapeDtypeStruct((rows, half), bf16),
            jax.ShapeDtypeStruct(args["state"].shape, f32),
        ),
        in_specs=[pl.BlockSpec(memory_space=pl.ANY)] * len(names),
        out_specs=(pl.BlockSpec(memory_space=pltpu.VMEM),) * 2,
        scratch_shapes=[V(a.shape, a.dtype) for a in args.values()]
        + [
            V((2, channels, groups * 2 * states), bf16),
            V((2, channels, groups * 2 * states), bf16),
            V((rows, channels), bf16),
            V((2, rows, channels), bf16),
            V((side, 2, rows, lanes), bf16),
            V((side, *din.shape), bf16),
            V((side, *dout.shape), bf16),
            V((chunks, side, rows, piece), bf16),
            V((side, rows, half), bf16),
            V((chunks, side, slots, piece), bf16),
            V((chunks, side, slots, piece), bf16),
            V((chunks, side, slots, piece), bf16),
            V((every, half), bf16),
            V((every, half), bf16),
            V((chunks, side, slots, piece), bf16),
            V((chunks, side, slots, piece), bf16),
            V((chunks, side, rows, piece), bf16),
            V((chunks, side, rows, piece), bf16),
            V((rows, half), bf16),
            V((rows, half), bf16),
            V((rows, 128), f32),
            V((rows, 128), f32),
            V((every, side * rows), bf16),
            V((side * rows, every), bf16),
            V((side * rows, half), f32),
            pltpu.SemaphoreType.DMA((len(names),)),
            pltpu.SemaphoreType.DMA((kinds, side)),
            pltpu.SemaphoreType.DMA((kinds, side)),
            pltpu.SemaphoreType.DMA((4 + chunks,)),
            pltpu.SemaphoreType.DMA((4 + chunks,)),
        ],
        compiler_params=pltpu.CompilerParams(
            collective_id=0, has_side_effects=True, vmem_limit_bytes=VMEM_BYTES
        ),
        name="layer",
    )(*args.values())


def body(
    layer_input,
    ssm_state,
    w_input,
    decay_rate,
    frequency,
    step_log,
    input_map,
    output_map,
    skip_gain,
    glu_weight,
    mix_out,
    norm_gain,
    norm_shift,
    route_ids,
    route_weights,
    gate_expert,
    up_expert,
    down_expert,
    gate_shared,
    up_shared,
    down_shared,
    dense_in,
    dense_out,
    branch_gate,
    final_gain,
    final_shift,
):
    count_ep = lax.axis_size("ep")
    count_tp = lax.axis_size("tp")
    seq_rows, width = layer_input.shape
    top_k = route_ids.shape[1]
    experts = gate_expert.shape[0] * count_ep
    cap = count_tp * max(1, min(seq_rows // count_tp, seq_rows * top_k // experts))
    side = math.isqrt(count_ep)
    layer_output, new_state = layer(
        side,
        cap,
        experts,
        dict(
            ids=route_ids.T,
            scores=route_weights.T,
            rate=decay_rate,
            freq=frequency,
            step=step_log[None],
            imap=input_map.transpose(0, 1, 3, 2),
            omap=output_map,
            skip=skip_gain,
            x=layer_input,
            win=w_input,
            state=ssm_state.reshape(-1, ssm_state.shape[3]),
            din=dense_in,
            dout=dense_out,
            glu=glu_weight,
            mix=mix_out,
            gain=norm_gain[None],
            shift=norm_shift[None],
            gs=gate_shared,
            us=up_shared,
            ds=down_shared,
            ge=gate_expert[0],
            ue=up_expert[0],
            de=down_expert[0],
            bgate=branch_gate[None],
            fgain=final_gain[None],
            fshift=final_shift[None],
        ),
    )
    new_state = new_state.reshape(ssm_state.shape)
    return (layer_output, new_state)


def solution(mesh):
    placed = (
        P(("grp", "ep"), None),
        P(None, ("grp", "ep"), "tp", None),
        P(None, "tp"),
        P("tp", None),
        P("tp", None),
        P("tp"),
        P(None, "tp", None, None),
        P(None, "tp", None, None),
        P("tp", None),
        P(),
        P(),
        P(),
        P(),
        P(("grp", "ep"), None),
        P(("grp", "ep"), None),
        P("ep", None, "tp"),
        P("ep", None, "tp"),
        P("ep", "tp", None),
        P(None, "tp"),
        P(None, "tp"),
        P("tp", None),
        P("ep", None),
        P("ep", "tp"),
        P(),
        P("tp"),
        P("tp"),
    )
    return jax.shard_map(
        body,
        mesh=mesh,
        in_specs=placed,
        out_specs=(P(("grp", "ep"), "tp"), P(None, ("grp", "ep"), "tp", None)),
        check_vma=False,
    )
```

```python
import functools
import math

import jax
import jax.numpy as jnp
from jax import lax
from jax.experimental import pallas as pl
from jax.experimental.pallas import tpu as pltpu
from jax.sharding import PartitionSpec as P

residual_alpha = 1.681792830507429
route_scale = 2.5
norm_eps = 1e-05
highest = lax.Precision.HIGHEST
MESH = pl.DeviceIdType.MESH
f32 = jnp.float32
bf16 = jnp.bfloat16
CHUNKS = 2
VMEM_BYTES = 64 * 1024 * 1024 - 1024 * 1024


def dot(a, b):
    return jnp.dot(a, b, preferred_element_type=f32)


def dot_t(a, b):
    return lax.dot_general(a, b, (((1,), (1,)), ((), ())), preferred_element_type=f32)


def iota(shape, dim):
    return lax.broadcasted_iota(jnp.int32, shape, dim).astype(f32)


def halves(a):
    high = a.astype(bf16)
    return high, (a - high.astype(f32)).astype(bf16)


def layer_kernel(side, cap, experts, names, *refs):
    count = len(names)
    hbm = refs[:count]
    out_ref, new_ref = refs[count : count + 2]
    local = dict(zip(names, refs[count + 2 :]))
    rest = refs[2 * count + 2 :]
    layer_steps(side, cap, experts, names, hbm, local, out_ref, new_ref, *rest)


def layer_steps(
    side,
    cap,
    experts,
    names,
    hbm,
    local,
    out_ref,
    new_ref,
    drive_v,
    omap_v,
    act_send,
    act_all,
    meta,
    din_all,
    dout_all,
    own_all,
    oth_all,
    x_send,
    x_recv,
    x_oth,
    y_send,
    y_oth,
    r_send,
    r_recv,
    s_send,
    s_recv,
    sh_send,
    sh_recv,
    st_send,
    st_recv,
    pick_v,
    mix_w,
    dense_v,
    load_sem,
    send_sem,
    recv_sem,
    tsend_sem,
    trecv_sem,
):
    x_ref, din_ref, dout_ref = local["x"], local["din"], local["dout"]
    rows, width = x_ref.shape
    half = width // 2
    chunks = own_all.shape[0]
    piece = half // chunks
    line_rows = side * rows
    slots = side * cap
    every = side * slots
    core = lax.axis_index("tp")
    chip = lax.axis_index("ep")
    row, col = lax.div(chip, side), lax.rem(chip, side)
    p = (1 - core) * col + core * row
    q = (1 - core) * row + core * col

    def chip_at(pp, qq):
        return (1 - core) * (qq * side + pp) + core * (pp * side + qq)

    def line_peer(d):
        pp = lax.rem(p + d + side, side)
        return pp, {"ep": chip_at(pp, q), "tp": core}

    def cross_peer(d):
        qq = lax.rem(q + d + side, side)
        return qq, {"ep": chip_at(p, qq), "tp": core}

    partner = {"ep": chip, "tp": 1 - core}
    tree = side == 8
    near = [d for d in (2, -2, 1, -1) if tree] or list(range(1, side))
    order = sorted(range(1, side), key=lambda d: -min(d, side - d))

    META, DIN, DOUT, OTH, OWN = 0, 1, 2, 3, 4
    XS, RS, SS = OWN + chunks, OWN + 2 * chunks, OWN + 3 * chunks

    def to_peer(kind, src, dst, place, device, me=None):
        if me is None:
            me = q if kind in (DIN, DOUT) or XS <= kind < SS else p
        return pltpu.make_async_remote_copy(
            src_ref=src,
            dst_ref=dst,
            send_sem=send_sem.at[kind, place],
            recv_sem=recv_sem.at[kind, me],
            device_id=device,
            device_id_type=MESH,
        )

    def arrived(kind, dst, place):
        pltpu.make_async_remote_copy(
            src_ref=dst,
            dst_ref=dst,
            send_sem=send_sem.at[kind, place],
            recv_sem=recv_sem.at[kind, place],
            device_id=partner,
            device_id_type=MESH,
        ).wait_recv()

    def to_partner(kind, src, dst):
        return pltpu.make_async_remote_copy(
            src_ref=src,
            dst_ref=dst,
            send_sem=tsend_sem.at[kind],
            recv_sem=trecv_sem.at[kind],
            device_id=partner,
            device_id_type=MESH,
        )

    def spread_out(kind, peer, me, src, dst):
        for d in near:
            place, device = peer(d)
            go(to_peer(kind, src, dst.at[me], place, device))

    def forward(kind, peer, me, dst):
        if not tree:
            return
        way = 1 - 2 * lax.rem(me, 2)
        for back, on, slot in ((-2, 1, 3), (2, -1, -3)):
            origin, _ = peer(back)
            arrived(kind, dst.at[origin], origin)
            _, device = peer(on)
            go(to_peer(kind, dst.at[origin], dst.at[origin], peer(slot)[0], device, origin))
        origin, _ = peer(-2 * way)
        _, device = peer(2 * way)
        go(to_peer(kind, dst.at[origin], dst.at[origin], peer(4)[0], device, origin))

    def rest_arrived(kind, peer, dst):
        for d in (1, -1, 3, -3, 4) if tree else near:
            place, _ = peer(d)
            arrived(kind, dst.at[place], place)

    sends = []

    def go(copy):
        copy.start()
        sends.append(copy)
        return copy

    loads = {
        name: pltpu.make_async_copy(src, local[name], load_sem.at[i])
        for i, (name, src) in enumerate(zip(names, hbm))
    }
    for load in loads.values():
        load.start()

    def loaded(*wanted):
        for name in wanted:
            loads[name].wait()

    barrier = pltpu.get_barrier_semaphore()
    pl.semaphore_signal(barrier, inc=1, device_id=partner, device_id_type=MESH)
    for d in range(1, side):
        for _, device in (line_peer(d), cross_peer(d)):
            pl.semaphore_signal(barrier, inc=1, device_id=device, device_id_type=MESH)

    lanes = meta.shape[2]
    loaded("ids", "scores")
    ids, scores = local["ids"][...].astype(f32), local["scores"][...]
    scores = scores / jnp.sum(scores, axis=0, keepdims=True) * route_scale
    eye = iota((rows, rows), 0) == iota((rows, rows), 1)
    lane = iota((rows, lanes), 1)
    hits = jnp.zeros((rows, lanes), f32)
    share = jnp.zeros((rows, lanes), f32)
    for k in range(ids.shape[0]):
        name = jnp.sum(jnp.where(eye, ids[k : k + 1], 0.0), axis=1, keepdims=True)
        score = jnp.sum(jnp.where(eye, scores[k : k + 1], 0.0), axis=1, keepdims=True)
        hits += jnp.where(lane == name, 1.0, 0.0)
        share += jnp.where(lane == name + experts, score, 0.0)
    earlier = jnp.where(iota((rows, rows), 1) < iota((rows, rows), 0), 1.0, 0.0)
    ranks = dot(earlier.astype(bf16), hits.astype(bf16))
    codes = jnp.where(hits > 0.5, ranks, -1.0)
    meta[p] = jnp.where(lane < experts, codes, share).astype(bf16)

    groups, states = local["rate"].shape
    members = local["skip"].shape[1]
    channels = groups * members
    pair = 2 * states
    drive_v[...] = jnp.zeros_like(drive_v)
    omap_v[...] = jnp.zeros_like(omap_v)
    loaded("rate", "freq", "step", "imap", "omap", "skip")
    rate, freq = local["rate"][...], local["freq"][...]
    eye = iota((groups, groups), 0) == iota((groups, groups), 1)
    step = jnp.exp(jnp.sum(jnp.where(eye, local["step"][...], 0.0), axis=1, keepdims=True))
    magnitude = jnp.exp(-rate * step)
    angle = freq * step
    decay_re, decay_im = magnitude * jnp.cos(angle), magnitude * jnp.sin(angle)
    denominator = rate * rate + freq * freq
    factor_re = ((decay_re - 1.0) * -rate + decay_im * freq) / denominator
    factor_im = (decay_im * -rate - (decay_re - 1.0) * freq) / denominator
    same = jnp.concatenate([decay_re, decay_re], axis=1)
    cross = jnp.concatenate([-decay_im, decay_im], axis=1)
    for g in range(groups):
        fr, fi = factor_re[g : g + 1], factor_im[g : g + 1]
        m0, m1 = local["imap"][0, g], local["imap"][1, g]
        drive = jnp.concatenate([fr * m0 - fi * m1, fr * m1 + fi * m0], axis=1)
        out = jnp.concatenate([local["omap"][0, g], -local["omap"][1, g]], axis=1)
        at, lanes_at = slice(g * members, (g + 1) * members), slice(g * pair, (g + 1) * pair)
        drive_v[0, at, lanes_at], drive_v[1, at, lanes_at] = halves(drive)
        omap_v[0, at, lanes_at], omap_v[1, at, lanes_at] = halves(out)
    tile = jnp.where(
        iota((members, channels), 0)
        == iota((members, channels), 1)
        - jnp.floor((iota((members, channels), 1) + 0.5) / members) * members,
        1.0,
        0.0,
    )
    skip = jnp.dot(local["skip"][...], tile, preferred_element_type=f32, precision=highest)
    in_group = jnp.floor((iota((groups, channels), 1) + 0.5) / members) == iota(
        (groups, channels), 0
    )
    skip = jnp.sum(jnp.where(in_group, skip, 0.0), axis=0, keepdims=True)
    loaded("x", "win")
    projected = dot(x_ref[...], local["win"][...]).astype(bf16)
    pushed = dot(projected, drive_v[0]) + dot(projected, drive_v[1])
    loaded("state")
    response = skip * projected.astype(f32)
    highs, lows = [], []
    for g in range(groups):
        old = jnp.concatenate(
            [
                local["state"][pl.ds(g, rows, stride=groups)],
                local["state"][pl.ds(rows * groups + g, rows, stride=groups)],
            ],
            axis=1,
        )
        turned = jnp.concatenate([old[:, states:], old[:, :states]], axis=1)
        new = same[g : g + 1] * old + cross[g : g + 1] * turned
        new += pushed[:, g * pair : (g + 1) * pair]
        new_ref[pl.ds(g, rows, stride=groups)] = new[:, :states]
        new_ref[pl.ds(rows * groups + g, rows, stride=groups)] = new[:, states:]
        high, low = halves(new)
        highs.append(high)
        lows.append(low)
    high, low = jnp.concatenate(highs, axis=1), jnp.concatenate(lows, axis=1)
    response += dot_t(high, omap_v[0]) + dot_t(high, omap_v[1]) + dot_t(low, omap_v[0])
    act_send[...] = jax.nn.gelu(response).astype(bf16)

    pl.semaphore_wait(barrier, 2 * side - 1)
    act_copy = go(to_partner(0, act_send, act_all.at[core]))
    act_all[core] = act_send[...]
    loaded("din", "dout")
    din_all[q] = din_ref[...]
    dout_all[q] = dout_ref[...]
    for d in order:
        place, device = line_peer(d)
        go(to_peer(META, meta.at[p], meta.at[p], place, device))
    spread_out(DIN, cross_peer, q, din_ref, din_all)
    spread_out(DOUT, cross_peer, q, dout_ref, dout_all)

    loaded("glu", "mix", "gain", "shift")
    glu_v, mix_v = local["glu"], local["mix"]
    act_copy.wait_recv()
    a0, a1 = act_all[0], act_all[1]
    gate = dot(a0, glu_v[:channels]) + dot(a1, glu_v[channels:])
    g0 = (a0.astype(f32) * jax.nn.sigmoid(gate[:, :channels])).astype(bf16)
    g1 = (a1.astype(f32) * jax.nn.sigmoid(gate[:, channels:])).astype(bf16)
    mixed = (dot(g0, mix_v[:channels]) + dot(g1, mix_v[channels:])).astype(bf16)
    values = residual_alpha * x_ref[...].astype(f32) + mixed.astype(f32)
    mean = jnp.mean(values, axis=1, keepdims=True)
    centred = values - mean
    variance = jnp.mean(centred * centred, axis=1, keepdims=True)
    normed = (centred * lax.rsqrt(variance + norm_eps) * local["gain"][...] + local["shift"][...]).astype(
        bf16
    )
    left, right = normed[:, :half], normed[:, half:]
    first = core == 0
    own = jnp.where(first, left, right)
    oth = jnp.where(first, right, left)
    for i in range(chunks):
        own_all[i, p] = own[:, i * piece : (i + 1) * piece]
    oth_all[p] = oth
    for i in range(chunks):
        spread_out(OWN + i, line_peer, p, own_all.at[i, p], own_all.at[i])

    for d in order:
        place, _ = line_peer(d)
        arrived(META, meta.at[place], place)
    lane = iota((1, every), 1)
    at_q = jnp.floor((lane + 0.5) / slots)
    at_p = jnp.floor((lane - at_q * slots + 0.5) / cap)
    at_rank = lane - at_q * slots - at_p * cap
    pf, cf = p.astype(f32), core.astype(f32)
    expert = (1.0 - cf) * (at_q * side + pf) + cf * (pf * side + at_q)
    at_lane = iota((lanes, every), 0)
    every_meta = meta[...].reshape(line_rows, lanes)
    codes = dot(every_meta, jnp.where(at_lane == expert, 1.0, 0.0).astype(bf16))
    shares = dot(every_meta, jnp.where(at_lane == expert + experts, 1.0, 0.0).astype(bf16))
    block = jnp.floor((iota((line_rows, 1), 0) + 0.5) / rows)
    chosen = jnp.where((codes == at_rank) & (block == at_p), 1.0, 0.0)
    mix_w[...] = (chosen * shares).astype(bf16)
    pick_v[...] = chosen.T.astype(bf16)

    forward(OWN, line_peer, p, own_all.at[0])

    loaded("gs", "us", "ds")
    gs_v, us_v, ds_v = local["gs"], local["us"], local["ds"]
    hidden = (jax.nn.silu(dot(normed, gs_v[...])) * dot(normed, us_v[...])).astype(bf16)
    base = core * half
    other = (1 - core) * half
    sh_send[...] = dot(hidden, ds_v[:, pl.ds(pl.multiple_of(other, 128), half)]).astype(bf16)
    shared_copy = go(to_partner(1, sh_send, sh_recv))
    shared_own = dot(hidden, ds_v[:, pl.ds(pl.multiple_of(base, 128), half)]).astype(bf16)

    for i in range(1, chunks):
        forward(OWN + i, line_peer, p, own_all.at[i])

    for i in range(chunks):
        rest_arrived(OWN + i, line_peer, own_all.at[i])
        picked = dot(pick_v[...], own_all[i].reshape(line_rows, piece)).astype(bf16)
        x_send[i] = picked.reshape(side, slots, piece)
        for d in order:
            place, device = cross_peer(d)
            go(to_peer(XS + i, x_send.at[i, place], x_recv.at[i, q], place, device))
        x_recv[i, q] = x_send[i, q]

    r0, r1 = iota((every, 1), 0), iota((1, every), 1)
    a = jnp.floor((r0 + 0.5) / slots)
    b = jnp.floor((r0 - a * slots + 0.5) / cap)
    swap = jnp.where(r1 == b * slots + a * cap + (r0 - a * slots - b * cap), 1.0, 0.0).astype(bf16)

    for i in range(chunks):
        for d in order:
            place, _ = cross_peer(d)
            arrived(XS + i, x_recv.at[i, place], place)
        go(to_partner(4 + i, x_recv.at[i], x_oth.at[i]))
    forward(DIN, cross_peer, q, din_all)
    forward(DOUT, cross_peer, q, dout_all)
    spread_out(OTH, line_peer, p, oth_all.at[p], oth_all)
    loaded("ge", "ue", "de")
    ge_v, ue_v, de_v = local["ge"], local["ue"], local["de"]
    units = ge_v.shape[1]
    gate = jnp.zeros((every, units), f32)
    up = jnp.zeros((every, units), f32)
    for i in range(chunks):
        tok = x_recv[i].reshape(every, piece)
        at = pl.ds(pl.multiple_of(base + i * piece, 128), piece)
        gate += dot(tok, ge_v[at])
        up += dot(tok, ue_v[at])
    for i in range(chunks):
        to_partner(4 + i, x_recv.at[i], x_oth.at[i]).wait_recv()
        tok = dot(swap, x_oth[i].reshape(every, piece)).astype(bf16)
        at = pl.ds(pl.multiple_of(other + i * piece, 128), piece)
        gate += dot(tok, ge_v[at])
        up += dot(tok, ue_v[at])
    hidden = (jax.nn.silu(gate) * up).astype(bf16)
    y_send[...] = dot(hidden, de_v[:, pl.ds(pl.multiple_of(other, 128), half)]).astype(bf16)
    y_copy = go(to_partner(2, y_send, y_oth))
    result = dot(hidden, de_v[:, pl.ds(pl.multiple_of(base, 128), half)])
    forward(OTH, line_peer, p, oth_all)
    y_copy.wait_recv()
    for i in range(chunks):
        at = slice(i * piece, (i + 1) * piece)
        theirs = dot(swap, y_oth[:, at])
        r_send[i] = (result[:, at] + theirs).astype(bf16).reshape(side, slots, piece)
        for d in order:
            place, device = cross_peer(d)
            go(to_peer(RS + i, r_send.at[i, place], r_recv.at[i, q], place, device))
        r_recv[i, q] = r_send[i, q]

    rest_arrived(OTH, line_peer, oth_all)
    rest_arrived(DIN, cross_peer, din_all)
    rest_arrived(DOUT, cross_peer, dout_all)
    units = side * din_ref.shape[0]
    din = din_all[...].reshape(units, width)
    din_left, din_right = din[:, :half], din[:, half:]
    din_own = jnp.where(first, din_left, din_right)
    din_oth = jnp.where(first, din_right, din_left)
    loaded("bgate")
    bgate = local["bgate"][...].astype(f32)
    bgate = jnp.concatenate([bgate[k : k + 1] for k in range(bgate.shape[0])], axis=1)
    bgate = jnp.broadcast_to(bgate, (8, width)).astype(bf16)
    b_own = jnp.where(first, bgate[:, :half], bgate[:, half:])
    b_oth = jnp.where(first, bgate[:, half:], bgate[:, :half])
    oth_tok = oth_all[...].reshape(line_rows, half)
    before = dot_t(oth_tok, din_oth)
    gate = dot_t(oth_tok, b_oth)
    for i in range(chunks):
        tok = own_all[i].reshape(line_rows, piece)
        before += dot_t(tok, din_own[:, i * piece : (i + 1) * piece])
        gate += dot_t(tok, b_own[:, i * piece : (i + 1) * piece])
    dense_hidden = jax.nn.gelu(before).astype(bf16)
    branch = jax.nn.sigmoid(gate[:, :1])
    dense_v[...] = branch * dot(dense_hidden, dout_all[...].reshape(units, half))

    for i in range(chunks):
        for d in order:
            place, _ = cross_peer(d)
            arrived(RS + i, r_recv.at[i, place], place)
        part = dot(mix_w[...], r_recv[i].reshape(every, piece))
        part += dense_v[:, i * piece : (i + 1) * piece]
        s_send[i] = part.astype(bf16).reshape(side, rows, piece)
        for d in order:
            place, device = line_peer(d)
            go(to_peer(SS + i, s_send.at[i, place], s_recv.at[i, p], place, device))
        s_recv[i, p] = s_send[i, p]

    shared_copy.wait_recv()
    shared = (shared_own.astype(f32) + sh_recv[...].astype(f32)).astype(bf16).astype(f32)
    skip = residual_alpha * own.astype(f32) + shared
    totals = []
    for i in range(chunks):
        for d in order:
            place, _ = line_peer(d)
            arrived(SS + i, s_recv.at[i, place], place)
        total = skip[:, i * piece : (i + 1) * piece]
        for j in range(side):
            total += s_recv[i, j].astype(f32)
        totals.append(total)
    loaded("fgain", "fshift")
    row_sum = sum(jnp.sum(t, axis=1, keepdims=True) for t in totals)
    row_squares = sum(jnp.sum(t * t, axis=1, keepdims=True) for t in totals)
    st_send[...] = jnp.where(iota(st_send.shape, 1) < 0.5, row_sum, row_squares)
    st_copy = go(to_partner(3, st_send, st_recv))
    st_copy.wait_recv()
    mean = (row_sum + st_recv[:, 0:1]) / width
    variance = (row_squares + st_recv[:, 1:2]) / width - mean * mean
    scale = lax.rsqrt(variance + norm_eps)
    for i in range(chunks):
        at = slice(i * piece, (i + 1) * piece)
        out_ref[:, at] = ((totals[i] - mean) * scale * local["fgain"][:, at] + local["fshift"][:, at]).astype(
            bf16
        )
    for copy in sends:
        copy.wait_send()


def layer(side, cap, experts, args):
    names = tuple(args)
    rows, width = args["x"].shape
    groups, states = args["rate"].shape
    channels = args["win"].shape[1]
    half = width // 2
    chunks = CHUNKS
    piece = half // chunks
    slots = side * cap
    every = side * slots
    lanes = -(-2 * experts // 128) * 128
    din, dout = args["din"], args["dout"]
    kinds = 4 + 4 * chunks
    V = pltpu.VMEM
    return pl.pallas_call(
        functools.partial(layer_kernel, side, cap, experts, names),
        out_shape=(
            jax.ShapeDtypeStruct((rows, half), bf16),
            jax.ShapeDtypeStruct(args["state"].shape, f32),
        ),
        in_specs=[pl.BlockSpec(memory_space=pl.ANY)] * len(names),
        out_specs=(pl.BlockSpec(memory_space=pltpu.VMEM),) * 2,
        scratch_shapes=[V(a.shape, a.dtype) for a in args.values()]
        + [
            V((2, channels, groups * 2 * states), bf16),
            V((2, channels, groups * 2 * states), bf16),
            V((rows, channels), bf16),
            V((2, rows, channels), bf16),
            V((side, rows, lanes), bf16),
            V((side, *din.shape), bf16),
            V((side, *dout.shape), bf16),
            V((chunks, side, rows, piece), bf16),
            V((side, rows, half), bf16),
            V((chunks, side, slots, piece), bf16),
            V((chunks, side, slots, piece), bf16),
            V((chunks, side, slots, piece), bf16),
            V((every, half), bf16),
            V((every, half), bf16),
            V((chunks, side, slots, piece), bf16),
            V((chunks, side, slots, piece), bf16),
            V((chunks, side, rows, piece), bf16),
            V((chunks, side, rows, piece), bf16),
            V((rows, half), bf16),
            V((rows, half), bf16),
            V((rows, 128), f32),
            V((rows, 128), f32),
            V((every, side * rows), bf16),
            V((side * rows, every), bf16),
            V((side * rows, half), f32),
            pltpu.SemaphoreType.DMA((len(names),)),
            pltpu.SemaphoreType.DMA((kinds, side)),
            pltpu.SemaphoreType.DMA((kinds, side)),
            pltpu.SemaphoreType.DMA((4 + chunks,)),
            pltpu.SemaphoreType.DMA((4 + chunks,)),
        ],
        compiler_params=pltpu.CompilerParams(
            collective_id=0, has_side_effects=True, vmem_limit_bytes=VMEM_BYTES
        ),
        name="layer",
    )(*args.values())


def body(
    layer_input,
    ssm_state,
    w_input,
    decay_rate,
    frequency,
    step_log,
    input_map,
    output_map,
    skip_gain,
    glu_weight,
    mix_out,
    norm_gain,
    norm_shift,
    route_ids,
    route_weights,
    gate_expert,
    up_expert,
    down_expert,
    gate_shared,
    up_shared,
    down_shared,
    dense_in,
    dense_out,
    branch_gate,
    final_gain,
    final_shift,
):
    count_ep = lax.axis_size("ep")
    count_tp = lax.axis_size("tp")
    seq_rows, width = layer_input.shape
    top_k = route_ids.shape[1]
    experts = gate_expert.shape[0] * count_ep
    cap = count_tp * max(1, min(seq_rows // count_tp, seq_rows * top_k // experts))
    side = math.isqrt(count_ep)
    layer_output, new_state = layer(
        side,
        cap,
        experts,
        dict(
            ids=route_ids.T,
            scores=route_weights.T,
            rate=decay_rate,
            freq=frequency,
            step=step_log[None],
            imap=input_map.transpose(0, 1, 3, 2),
            omap=output_map,
            skip=skip_gain,
            x=layer_input,
            win=w_input,
            state=ssm_state.reshape(-1, ssm_state.shape[3]),
            din=dense_in,
            dout=dense_out,
            glu=glu_weight,
            mix=mix_out,
            gain=norm_gain[None],
            shift=norm_shift[None],
            gs=gate_shared,
            us=up_shared,
            ds=down_shared,
            ge=gate_expert[0],
            ue=up_expert[0],
            de=down_expert[0],
            bgate=branch_gate.reshape(-1, 128),
            fgain=final_gain[None],
            fshift=final_shift[None],
        ),
    )
    new_state = new_state.reshape(ssm_state.shape)
    return (layer_output, new_state)


def solution(mesh):
    placed = (
        P(("grp", "ep"), None),
        P(None, ("grp", "ep"), "tp", None),
        P(None, "tp"),
        P("tp", None),
        P("tp", None),
        P("tp"),
        P(None, "tp", None, None),
        P(None, "tp", None, None),
        P("tp", None),
        P(),
        P(),
        P(),
        P(),
        P(("grp", "ep"), None),
        P(("grp", "ep"), None),
        P("ep", None, "tp"),
        P("ep", None, "tp"),
        P("ep", "tp", None),
        P(None, "tp"),
        P(None, "tp"),
        P("tp", None),
        P("ep", None),
        P("ep", "tp"),
        P(),
        P("tp"),
        P("tp"),
    )
    return jax.shard_map(
        body,
        mesh=mesh,
        in_specs=placed,
        out_specs=(P(("grp", "ep"), "tp"), P(None, ("grp", "ep"), "tp", None)),
        check_vma=False,
    )
```

```python
import functools
import math

import jax
import jax.numpy as jnp
from jax import lax
from jax.experimental import pallas as pl
from jax.experimental.pallas import tpu as pltpu
from jax.sharding import PartitionSpec as P

residual_alpha = 1.681792830507429
route_scale = 2.5
norm_eps = 1e-05
highest = lax.Precision.HIGHEST
MESH = pl.DeviceIdType.MESH
f32 = jnp.float32
bf16 = jnp.bfloat16
VMEM_BYTES = 64 * 1024 * 1024 - 1024 * 1024


def dot(a, b):
    return jnp.dot(a, b, preferred_element_type=f32)


def dot_t(a, b):
    return lax.dot_general(a, b, (((1,), (1,)), ((), ())), preferred_element_type=f32)


def iota(shape, dim):
    return lax.broadcasted_iota(jnp.int32, shape, dim).astype(f32)


def halves(a):
    high = a.astype(bf16)
    return high, (a - high.astype(f32)).astype(bf16)


def layer_kernel(side, cap, experts, names, *refs):
    count = len(names)
    hbm = refs[:count]
    out_ref, new_ref = refs[count : count + 2]
    local = dict(zip(names, refs[count + 2 :]))
    rest = refs[2 * count + 2 :]
    layer_steps(side, cap, experts, names, hbm, local, out_ref, new_ref, *rest)


def layer_steps(
    side,
    cap,
    experts,
    names,
    hbm,
    local,
    out_ref,
    new_ref,
    drive_v,
    omap_v,
    act_send,
    act_all,
    meta,
    din_all,
    dout_all,
    own_all,
    oth_all,
    x_send,
    x_recv,
    x_oth,
    y_send,
    y_oth,
    r_send,
    r_recv,
    s_send,
    s_recv,
    relay,
    merged,
    sh_send,
    sh_recv,
    st_send,
    st_recv,
    pick_v,
    mix_w,
    dense_v,
    load_sem,
    send_sem,
    recv_sem,
    tsend_sem,
    trecv_sem,
):
    x_ref, din_ref, dout_ref = local["x"], local["din"], local["dout"]
    rows, width = x_ref.shape
    half = width // 2
    line_rows = side * rows
    group = side // 2
    slots = group * cap
    part_rows = side * slots
    every = 2 * part_rows
    core = lax.axis_index("tp")
    chip = lax.axis_index("ep")
    row, col = lax.div(chip, side), lax.rem(chip, side)
    p = (1 - core) * col + core * row
    q = (1 - core) * row + core * col

    def chip_at(pp, qq):
        return (1 - core) * (qq * side + pp) + core * (pp * side + qq)

    def slot(d):
        d = (d + side - 1) % side
        d = d + 1 - side if d + 1 > side // 2 else d + 1
        return 2 * d - 1 if d > 0 else -2 * d

    def line_peer(d):
        return {"ep": chip_at(lax.rem(p + d + side, side), q), "tp": core}

    def cross_peer(d):
        return {"ep": chip_at(p, lax.rem(q + d + side, side)), "tp": core}

    partner = {"ep": chip, "tp": 1 - core}
    tree = side == 8
    near = [d for d in (2, -2, 1, -1) if tree] or list(range(1, side))
    order = sorted(range(1, side), key=lambda d: -min(d, side - d))
    if tree:
        order = [4, 3, -3, 2, -2, 1, -1]

    META, DIN, DOUT, OTH, OWN, XS, RS, SS = 0, 1, 2, 3, 4, 5, 7, 9

    def send(kind, device, src, dst, sent, landed):
        go(
            pltpu.make_async_remote_copy(
                src_ref=src,
                dst_ref=dst,
                send_sem=send_sem.at[kind, sent],
                recv_sem=recv_sem.at[kind, landed],
                device_id=device,
                device_id_type=MESH,
            )
        )

    def arrived(kind, dst, landed):
        pltpu.make_async_remote_copy(
            src_ref=dst,
            dst_ref=dst,
            send_sem=send_sem.at[kind, landed],
            recv_sem=recv_sem.at[kind, landed],
            device_id=partner,
            device_id_type=MESH,
        ).wait_recv()

    def to_partner(kind, src, dst):
        return pltpu.make_async_remote_copy(
            src_ref=src,
            dst_ref=dst,
            send_sem=tsend_sem.at[kind],
            recv_sem=trecv_sem.at[kind],
            device_id=partner,
            device_id_type=MESH,
        )

    def spread_out(kind, peer, dst, offsets):
        for d in offsets:
            send(kind, peer(d), dst.at[0], dst.at[slot(-d)], slot(d), slot(-d))

    def forward(kind, peer, dst, place):
        if not tree:
            return
        for back, on in ((-2, 1), (2, -1)):
            arrived(kind, dst.at[slot(back)], slot(back))
            to = slot(back - on)
            send(kind, peer(on), dst.at[slot(back)], dst.at[to], slot(on - back), to)
        way = 1 - 2 * lax.rem(place, 2)
        middle = lax.div(7 + way, 2)
        send(kind, peer(2 * way), dst.at[middle], dst.at[slot(4)], slot(4), slot(4))

    def rest_arrived(kind, dst, offsets):
        for d in offsets:
            arrived(kind, dst.at[slot(d)], slot(d))

    beyond = [1, -1, 3, -3, 4] if tree else near

    sends = []

    def go(copy):
        copy.start()
        sends.append(copy)
        return copy

    loads = {
        name: pltpu.make_async_copy(src, local[name], load_sem.at[i])
        for i, (name, src) in enumerate(zip(names, hbm))
    }
    later = names.index("din")
    for name in names[:later]:
        loads[name].start()
    barrier = pltpu.get_barrier_semaphore()
    pl.semaphore_signal(barrier, inc=1, device_id=partner, device_id_type=MESH)
    for d in range(1, side):
        for device in (line_peer(d), cross_peer(d)):
            pl.semaphore_signal(barrier, inc=1, device_id=device, device_id_type=MESH)
    for name in names[later:]:
        loads[name].start()

    def loaded(*wanted):
        for name in wanted:
            loads[name].wait()

    groups, states = local["rate"].shape
    members = local["skip"].shape[1]
    channels = groups * members
    pair = 2 * states
    drive_v[...] = jnp.zeros_like(drive_v)
    omap_v[...] = jnp.zeros_like(omap_v)
    loaded("rate", "freq", "step", "imap", "omap", "skip")
    rate, freq = local["rate"][...], local["freq"][...]
    eye = iota((groups, groups), 0) == iota((groups, groups), 1)
    step = jnp.exp(jnp.sum(jnp.where(eye, local["step"][...], 0.0), axis=1, keepdims=True))
    magnitude = jnp.exp(-rate * step)
    angle = freq * step
    decay_re, decay_im = magnitude * jnp.cos(angle), magnitude * jnp.sin(angle)
    denominator = rate * rate + freq * freq
    factor_re = ((decay_re - 1.0) * -rate + decay_im * freq) / denominator
    factor_im = (decay_im * -rate - (decay_re - 1.0) * freq) / denominator
    same = jnp.concatenate([decay_re, decay_re], axis=1)
    cross = jnp.concatenate([-decay_im, decay_im], axis=1)
    for g in range(groups):
        fr, fi = factor_re[g : g + 1], factor_im[g : g + 1]
        m0, m1 = local["imap"][0, g], local["imap"][1, g]
        drive = jnp.concatenate([fr * m0 - fi * m1, fr * m1 + fi * m0], axis=1)
        out = jnp.concatenate([local["omap"][0, g], -local["omap"][1, g]], axis=1)
        at, lanes_at = slice(g * members, (g + 1) * members), slice(g * pair, (g + 1) * pair)
        drive_v[0, at, lanes_at], drive_v[1, at, lanes_at] = halves(drive)
        omap_v[at, lanes_at] = out.astype(bf16)
    tile = jnp.where(
        iota((members, channels), 0)
        == iota((members, channels), 1)
        - jnp.floor((iota((members, channels), 1) + 0.5) / members) * members,
        1.0,
        0.0,
    )
    skip = jnp.dot(local["skip"][...], tile, preferred_element_type=f32, precision=highest)
    in_group = jnp.floor((iota((groups, channels), 1) + 0.5) / members) == iota(
        (groups, channels), 0
    )
    skip = jnp.sum(jnp.where(in_group, skip, 0.0), axis=0, keepdims=True)
    loaded("x", "win")
    projected = dot(x_ref[...], local["win"][...]).astype(bf16)
    pushed = dot(projected, drive_v[0]) + dot(projected, drive_v[1])
    loaded("state")
    response = skip * projected.astype(f32)
    states_now = []
    for g in range(groups):
        old = jnp.concatenate(
            [
                local["state"][pl.ds(g, rows, stride=groups)],
                local["state"][pl.ds(rows * groups + g, rows, stride=groups)],
            ],
            axis=1,
        )
        turned = jnp.concatenate([old[:, states:], old[:, :states]], axis=1)
        new = same[g : g + 1] * old + cross[g : g + 1] * turned
        new += pushed[:, g * pair : (g + 1) * pair]
        new_ref[pl.ds(g, rows, stride=groups)] = new[:, :states]
        new_ref[pl.ds(rows * groups + g, rows, stride=groups)] = new[:, states:]
        states_now.append(new.astype(bf16))
    response += dot_t(jnp.concatenate(states_now, axis=1), omap_v[...])
    act_send[...] = jax.nn.gelu(response).astype(bf16)

    pl.semaphore_wait(barrier, 2 * side - 1)
    act_copy = go(to_partner(0, act_send, act_all.at[core]))
    act_all[core] = act_send[...]
    loaded("din", "dout")
    din_all[0] = din_ref[...]
    dout_all[0] = dout_ref[...]
    spread_out(DIN, cross_peer, din_all, near)
    spread_out(DOUT, cross_peer, dout_all, near)

    lanes = meta.shape[2]
    loaded("ids", "scores")
    ids, scores = local["ids"][...].astype(f32), local["scores"][...]
    scores = scores / jnp.sum(scores, axis=0, keepdims=True) * route_scale
    eye = iota((rows, rows), 0) == iota((rows, rows), 1)
    lane = iota((rows, lanes), 1)
    hits = jnp.zeros((rows, lanes), f32)
    share = jnp.zeros((rows, lanes), f32)
    for k in range(ids.shape[0]):
        name = jnp.sum(jnp.where(eye, ids[k : k + 1], 0.0), axis=1, keepdims=True)
        score = jnp.sum(jnp.where(eye, scores[k : k + 1], 0.0), axis=1, keepdims=True)
        hits += jnp.where(lane == name, 1.0, 0.0)
        share += jnp.where(lane == name + experts, score, 0.0)
    earlier = jnp.where(iota((rows, rows), 1) < iota((rows, rows), 0), 1.0, 0.0)
    ranks = dot(earlier.astype(bf16), hits.astype(bf16))
    codes = jnp.where(hits > 0.5, ranks, -1.0)
    meta[0] = jnp.where(lane < experts, codes, share).astype(bf16)
    spread_out(META, line_peer, meta, order)

    loaded("glu", "mix", "gain", "shift")
    glu_v, mix_v = local["glu"], local["mix"]
    act_copy.wait_recv()
    a0, a1 = act_all[0], act_all[1]
    gate = dot(a0, glu_v[:channels]) + dot(a1, glu_v[channels:])
    g0 = (a0.astype(f32) * jax.nn.sigmoid(gate[:, :channels])).astype(bf16)
    g1 = (a1.astype(f32) * jax.nn.sigmoid(gate[:, channels:])).astype(bf16)
    mixed = (dot(g0, mix_v[:channels]) + dot(g1, mix_v[channels:])).astype(bf16)
    values = residual_alpha * x_ref[...].astype(f32) + mixed.astype(f32)
    mean = jnp.mean(values, axis=1, keepdims=True)
    centred = values - mean
    variance = jnp.mean(centred * centred, axis=1, keepdims=True)
    normed = (centred * lax.rsqrt(variance + norm_eps) * local["gain"][...] + local["shift"][...]).astype(
        bf16
    )
    left, right = normed[:, :half], normed[:, half:]
    first = core == 0
    own = jnp.where(first, left, right)
    oth = jnp.where(first, right, left)
    own_all[0] = own
    oth_all[0] = oth
    spread_out(OWN, line_peer, own_all, near)

    rest_arrived(META, meta, order)

    def steps(index):
        odd = index - 2.0 * jnp.floor((index + 0.5) / 2.0)
        ahead = jnp.floor((index + 1.5) / 2.0)
        return jnp.where(odd > 0.5, ahead, -ahead)

    def parts_of(index):
        part = jnp.floor((index + 0.5) / part_rows)
        index = index - part * part_rows
        cross_slot = jnp.floor((index + 0.5) / slots)
        index = index - cross_slot * slots
        member = jnp.floor((index + 0.5) / cap)
        return cross_slot, part * group + member, index - member * cap

    cross_slot, line_slot, at_rank = parts_of(iota((1, every), 1))
    pf, qf, cf = p.astype(f32), q.astype(f32), core.astype(f32)
    at_q = qf + steps(cross_slot)
    at_q = at_q - side * jnp.floor((at_q + 0.5) / side)
    expert = (1.0 - cf) * (at_q * side + pf) + cf * (pf * side + at_q)
    at_lane = iota((lanes, every), 0)
    every_meta = meta[...].reshape(line_rows, lanes)
    codes = dot(every_meta, jnp.where(at_lane == expert, 1.0, 0.0).astype(bf16))
    shares = dot(every_meta, jnp.where(at_lane == expert + experts, 1.0, 0.0).astype(bf16))
    block = jnp.floor((iota((line_rows, 1), 0) + 0.5) / rows)
    chosen = jnp.where((codes == at_rank) & (block == line_slot), 1.0, 0.0)
    weighted = (chosen * shares).astype(bf16)
    part_tokens = group * rows
    for h in range(2):
        tokens = slice(h * part_tokens, (h + 1) * part_tokens)
        lanes_at = slice(h * part_rows, (h + 1) * part_rows)
        mix_w[h] = weighted[tokens, lanes_at]
        pick_v[h] = chosen[tokens, lanes_at].T.astype(bf16)

    forward(OWN, line_peer, own_all, p)

    loaded("gs", "us", "ds")
    gs_v, us_v, ds_v = local["gs"], local["us"], local["ds"]
    hidden = (jax.nn.silu(dot(normed, gs_v[...])) * dot(normed, us_v[...])).astype(bf16)
    base = core * half
    other = (1 - core) * half
    sh_send[...] = dot(hidden, ds_v[:, pl.ds(pl.multiple_of(other, 128), half)]).astype(bf16)
    shared_copy = go(to_partner(1, sh_send, sh_recv))
    shared_own = dot(hidden, ds_v[:, pl.ds(pl.multiple_of(base, 128), half)]).astype(bf16)

    for h in range(2):
        first_ones = [1, -1] if h == 0 else [3, -3, 4]
        if not tree:
            first_ones = [d for d in near if slot(d) // group == h]
        rest_arrived(OWN, own_all, first_ones)
        tokens = own_all[h * group : (h + 1) * group].reshape(part_tokens, half)
        x_send[h] = dot(pick_v[h], tokens).astype(bf16).reshape(side, slots, half)
        for d in order:
            place = slot(d)
            send(
                XS + h, cross_peer(d), x_send.at[h, place], x_recv.at[h, slot(-d)], place, slot(-d)
            )
        x_recv[h, 0] = x_send[h, 0]

    mine = parts_of(iota((every, 1), 0))
    theirs = parts_of(iota((1, every), 1))
    swap = jnp.where(
        (mine[0] == theirs[1]) & (mine[1] == theirs[0]) & (mine[2] == theirs[2]), 1.0, 0.0
    ).astype(bf16)

    for h in range(2):
        for d in order:
            arrived(XS + h, x_recv.at[h, slot(d)], slot(d))
        go(to_partner(4 + h, x_recv.at[h], x_oth.at[h]))
    spread_out(OTH, line_peer, oth_all, near)
    forward(DIN, cross_peer, din_all, q)
    forward(DOUT, cross_peer, dout_all, q)
    loaded("ge", "ue", "de")
    ge_v, ue_v, de_v = local["ge"], local["ue"], local["de"]
    tok = x_recv[...].reshape(every, half)
    at = pl.ds(pl.multiple_of(base, 128), half)
    gate, up = dot(tok, ge_v[at]), dot(tok, ue_v[at])
    for h in range(2):
        to_partner(4 + h, x_recv.at[h], x_oth.at[h]).wait_recv()
    tok = dot(swap, x_oth[...].reshape(every, half)).astype(bf16)
    at = pl.ds(pl.multiple_of(other, 128), half)
    gate += dot(tok, ge_v[at])
    up += dot(tok, ue_v[at])
    hidden = (jax.nn.silu(gate) * up).astype(bf16)
    down_own = de_v[:, pl.ds(pl.multiple_of(base, 128), half)]
    down_other = de_v[:, pl.ds(pl.multiple_of(other, 128), half)]
    for_partner = dot(swap, hidden).astype(bf16)
    for h in (1, 0):
        at = slice(h * part_rows, (h + 1) * part_rows)
        y_send[h] = dot(for_partner[at], down_other).astype(bf16)
        go(to_partner(2 if h else 6, y_send.at[h], y_oth.at[h]))
    result = dot(hidden, down_own)
    for h in (1, 0):
        to_partner(2 if h else 6, y_send.at[h], y_oth.at[h]).wait_recv()
        at = slice(h * part_rows, (h + 1) * part_rows)
        total = result[at] + y_oth[h].astype(f32)
        r_send[h] = total.astype(bf16).reshape(side, slots, half)
        for d in order:
            place = slot(d)
            send(
                RS + h, cross_peer(d), r_send.at[h, place], r_recv.at[h, slot(-d)], place, slot(-d)
            )
        r_recv[h, 0] = r_send[h, 0]
        if h:
            forward(OTH, line_peer, oth_all, p)

    rest_arrived(OTH, oth_all, beyond)
    rest_arrived(DIN, din_all, beyond)
    rest_arrived(DOUT, dout_all, beyond)
    units = side * din_ref.shape[0]
    din = din_all[...].reshape(units, width)
    din_left, din_right = din[:, :half], din[:, half:]
    din_own = jnp.where(first, din_left, din_right)
    din_oth = jnp.where(first, din_right, din_left)
    loaded("bgate")
    bgate = local["bgate"][...].astype(f32)
    bgate = jnp.concatenate([bgate[k : k + 1] for k in range(bgate.shape[0])], axis=1)
    bgate = jnp.broadcast_to(bgate, (8, width)).astype(bf16)
    b_own = jnp.where(first, bgate[:, :half], bgate[:, half:])
    b_oth = jnp.where(first, bgate[:, half:], bgate[:, :half])
    oth_tok = oth_all[...].reshape(line_rows, half)
    own_tok = own_all[...].reshape(line_rows, half)
    before = dot_t(oth_tok, din_oth) + dot_t(own_tok, din_own)
    gate = dot_t(oth_tok, b_oth) + dot_t(own_tok, b_own)
    dense_hidden = jax.nn.gelu(before).astype(bf16)
    branch = jax.nn.sigmoid(gate[:, :1])
    dense_v[...] = branch * dot(dense_hidden, dout_all[...].reshape(units, half))

    def send_sum(on, src, dst, sent, landed):
        send(SS, line_peer(on), src, dst, sent, landed)

    way = 1 - 2 * lax.rem(p, 2)
    for h in (1, 0):
        for d in order:
            arrived(RS + h, r_recv.at[h, slot(d)], slot(d))
        tokens = slice(h * part_tokens, (h + 1) * part_tokens)
        part = dot(mix_w[h], r_recv[h].reshape(part_rows, half)) + dense_v[tokens]
        s_send[h * group : (h + 1) * group] = part.astype(bf16).reshape(group, rows, half)
        if not tree:
            for d in order:
                if slot(d) // group == h:
                    send_sum(d, s_send.at[slot(d)], s_recv.at[slot(-d)], slot(d), slot(-d))
        elif h:
            send_sum(-2 * way, s_send.at[slot(4)], relay.at[2], slot(4), slot(4))
            send_sum(-1, s_send.at[slot(-3)], relay.at[0], slot(-3), slot(3))
            send_sum(1, s_send.at[slot(3)], relay.at[1], slot(3), slot(-3))
        else:
            for d in (1, -1):
                send_sum(d, s_send.at[slot(d)], s_recv.at[slot(-d)], slot(d), slot(-d))
    if tree:
        for k, d in enumerate((3, -3, 4)):
            arrived(SS, relay.at[k], slot(d))
        third = relay[2].astype(f32)
        for k, d in enumerate((-2, 2)):
            mine = s_send[slot(d)].astype(f32) + relay[k].astype(f32)
            mine += jnp.where(d * way < 0, third, 0.0)
            merged[k] = mine.astype(bf16)
            send_sum(d, merged.at[k], s_recv.at[slot(-d)], slot(d), slot(-d))

    shared_copy.wait_recv()
    shared = (shared_own.astype(f32) + sh_recv[...].astype(f32)).astype(bf16).astype(f32)
    skip = residual_alpha * own.astype(f32) + shared
    total = skip + s_send[0].astype(f32)
    for d in near:
        arrived(SS, s_recv.at[slot(d)], slot(d))
        total += s_recv[slot(d)].astype(f32)
    loaded("fgain", "fshift")
    row_sum = jnp.sum(total, axis=1, keepdims=True)
    row_squares = jnp.sum(total * total, axis=1, keepdims=True)
    st_send[...] = jnp.where(iota(st_send.shape, 1) < 0.5, row_sum, row_squares)
    st_copy = go(to_partner(3, st_send, st_recv))
    st_copy.wait_recv()
    mean = (row_sum + st_recv[:, 0:1]) / width
    variance = (row_squares + st_recv[:, 1:2]) / width - mean * mean
    scale = lax.rsqrt(variance + norm_eps)
    out = (total - mean) * scale * local["fgain"][...] + local["fshift"][...]
    out_ref[...] = out.astype(bf16)
    for copy in sends:
        copy.wait_send()


def layer(side, cap, experts, args):
    names = tuple(args)
    rows, width = args["x"].shape
    groups, states = args["rate"].shape
    channels = args["win"].shape[1]
    half = width // 2
    group = side // 2
    slots = group * cap
    part_rows = side * slots
    every = 2 * part_rows
    lanes = -(-2 * experts // 128) * 128
    din, dout = args["din"], args["dout"]
    kinds = 10
    V = pltpu.VMEM
    return pl.pallas_call(
        functools.partial(layer_kernel, side, cap, experts, names),
        out_shape=(
            pltpu.VMEM((rows, half), bf16),
            pltpu.VMEM(args["state"].shape, f32),
        ),
        in_specs=[pl.BlockSpec(memory_space=pl.ANY)] * len(names),
        out_specs=(pl.BlockSpec(memory_space=pltpu.VMEM),) * 2,
        scratch_shapes=[V(a.shape, a.dtype) for a in args.values()]
        + [
            V((2, channels, groups * 2 * states), bf16),
            V((channels, groups * 2 * states), bf16),
            V((rows, channels), bf16),
            V((2, rows, channels), bf16),
            V((side, rows, lanes), bf16),
            V((side, *din.shape), bf16),
            V((side, *dout.shape), bf16),
            V((side, rows, half), bf16),
            V((side, rows, half), bf16),
            V((2, side, slots, half), bf16),
            V((2, side, slots, half), bf16),
            V((2, side, slots, half), bf16),
            V((2, part_rows, half), bf16),
            V((2, part_rows, half), bf16),
            V((2, side, slots, half), bf16),
            V((2, side, slots, half), bf16),
            V((side, rows, half), bf16),
            V((side, rows, half), bf16),
            V((3, rows, half), bf16),
            V((2, rows, half), bf16),
            V((rows, half), bf16),
            V((rows, half), bf16),
            V((rows, 128), f32),
            V((rows, 128), f32),
            V((2, part_rows, group * rows), bf16),
            V((2, group * rows, part_rows), bf16),
            V((side * rows, half), f32),
            pltpu.SemaphoreType.DMA((len(names),)),
            pltpu.SemaphoreType.DMA((kinds, side)),
            pltpu.SemaphoreType.DMA((kinds, side)),
            pltpu.SemaphoreType.DMA((7,)),
            pltpu.SemaphoreType.DMA((7,)),
        ],
        compiler_params=pltpu.CompilerParams(
            collective_id=0, has_side_effects=True, vmem_limit_bytes=VMEM_BYTES
        ),
        name="layer",
    )(*args.values())


def body(
    layer_input,
    ssm_state,
    w_input,
    decay_rate,
    frequency,
    step_log,
    input_map,
    output_map,
    skip_gain,
    glu_weight,
    mix_out,
    norm_gain,
    norm_shift,
    route_ids,
    route_weights,
    gate_expert,
    up_expert,
    down_expert,
    gate_shared,
    up_shared,
    down_shared,
    dense_in,
    dense_out,
    branch_gate,
    final_gain,
    final_shift,
):
    count_ep = lax.axis_size("ep")
    count_tp = lax.axis_size("tp")
    seq_rows, width = layer_input.shape
    top_k = route_ids.shape[1]
    experts = gate_expert.shape[0] * count_ep
    cap = count_tp * max(1, min(seq_rows // count_tp, seq_rows * top_k // experts))
    side = math.isqrt(count_ep)
    layer_output, new_state = layer(
        side,
        cap,
        experts,
        dict(
            ids=route_ids.T,
            scores=route_weights.T,
            rate=decay_rate,
            freq=frequency,
            step=step_log[None],
            imap=input_map.transpose(0, 1, 3, 2),
            omap=output_map,
            skip=skip_gain,
            x=layer_input,
            win=w_input,
            state=ssm_state.reshape(-1, ssm_state.shape[3]),
            din=dense_in,
            dout=dense_out,
            glu=glu_weight,
            mix=mix_out,
            gain=norm_gain[None],
            shift=norm_shift[None],
            gs=gate_shared,
            us=up_shared,
            ds=down_shared,
            ge=gate_expert[0],
            ue=up_expert[0],
            de=down_expert[0],
            bgate=branch_gate.reshape(-1, 128),
            fgain=final_gain[None],
            fshift=final_shift[None],
        ),
    )
    new_state = new_state.reshape(ssm_state.shape)
    return (layer_output, new_state)


def solution(mesh):
    placed = (
        P(("grp", "ep"), None),
        P(None, ("grp", "ep"), "tp", None),
        P(None, "tp"),
        P("tp", None),
        P("tp", None),
        P("tp"),
        P(None, "tp", None, None),
        P(None, "tp", None, None),
        P("tp", None),
        P(),
        P(),
        P(),
        P(),
        P(("grp", "ep"), None),
        P(("grp", "ep"), None),
        P("ep", None, "tp"),
        P("ep", None, "tp"),
        P("ep", "tp", None),
        P(None, "tp"),
        P(None, "tp"),
        P("tp", None),
        P("ep", None),
        P("ep", "tp"),
        P(),
        P("tp"),
        P("tp"),
    )
    return jax.shard_map(
        body,
        mesh=mesh,
        in_specs=placed,
        out_specs=(P(("grp", "ep"), "tp"), P(None, ("grp", "ep"), "tp", None)),
        check_vma=False,
    )
```

```python
import functools
import math

import jax
import jax.numpy as jnp
from jax import lax
from jax.experimental import pallas as pl
from jax.experimental.pallas import tpu as pltpu
from jax.sharding import PartitionSpec as P

residual_alpha = 1.681792830507429
route_scale = 2.5
norm_eps = 1e-05
highest = lax.Precision.HIGHEST
MESH = pl.DeviceIdType.MESH
f32 = jnp.float32
bf16 = jnp.bfloat16
VMEM_BYTES = 64 * 1024 * 1024 - 1024 * 1024


def dot(a, b):
    return jnp.dot(a, b, preferred_element_type=f32)


def dot_t(a, b):
    return lax.dot_general(a, b, (((1,), (1,)), ((), ())), preferred_element_type=f32)


def iota(shape, dim):
    return lax.broadcasted_iota(jnp.int32, shape, dim).astype(f32)


def halves(a):
    high = a.astype(bf16)
    return high, (a - high.astype(f32)).astype(bf16)


def layer_kernel(side, cap, experts, names, *refs):
    count = len(names)
    hbm = refs[:count]
    out_ref, new_ref = refs[count : count + 2]
    local = dict(zip(names, refs[count + 2 :]))
    rest = refs[2 * count + 2 :]
    layer_steps(side, cap, experts, names, hbm, local, out_ref, new_ref, *rest)


def layer_steps(
    side,
    cap,
    experts,
    names,
    hbm,
    local,
    out_ref,
    new_ref,
    drive_v,
    omap_v,
    act_send,
    act_all,
    meta,
    din_all,
    dout_all,
    own_all,
    oth_all,
    x_send,
    x_recv,
    x_oth,
    y_send,
    y_oth,
    r_send,
    r_recv,
    s_send,
    s_recv,
    relay,
    merged,
    sh_send,
    sh_recv,
    st_send,
    st_recv,
    pick_v,
    mix_w,
    dense_v,
    load_sem,
    send_sem,
    recv_sem,
    tsend_sem,
    trecv_sem,
):
    x_ref, din_ref, dout_ref = local["x"], local["din"], local["dout"]
    rows, width = x_ref.shape
    half = width // 2
    line_rows = side * rows
    group = side // 2
    slots = group * cap
    part_rows = side * slots
    every = 2 * part_rows
    core = lax.axis_index("tp")
    chip = lax.axis_index("ep")
    row, col = lax.div(chip, side), lax.rem(chip, side)
    p = (1 - core) * col + core * row
    q = (1 - core) * row + core * col

    def chip_at(pp, qq):
        return (1 - core) * (qq * side + pp) + core * (pp * side + qq)

    def slot(d):
        d = (d + side - 1) % side
        d = d + 1 - side if d + 1 > side // 2 else d + 1
        return 2 * d - 1 if d > 0 else -2 * d

    def line_peer(d):
        return {"ep": chip_at(lax.rem(p + d + side, side), q), "tp": core}

    def cross_peer(d):
        return {"ep": chip_at(p, lax.rem(q + d + side, side)), "tp": core}

    partner = {"ep": chip, "tp": 1 - core}
    tree = side == 8
    near = [d for d in (2, -2, 1, -1) if tree] or list(range(1, side))
    order = sorted(range(1, side), key=lambda d: -min(d, side - d))
    if tree:
        order = [4, 3, -3, 2, -2, 1, -1]

    META, DIN, DOUT, OTH, OWN, XS, RS, SS = 0, 1, 2, 3, 4, 5, 7, 9

    def send(kind, device, src, dst, sent, landed):
        go(
            pltpu.make_async_remote_copy(
                src_ref=src,
                dst_ref=dst,
                send_sem=send_sem.at[kind, sent],
                recv_sem=recv_sem.at[kind, landed],
                device_id=device,
                device_id_type=MESH,
            )
        )

    def arrived(kind, dst, landed):
        pltpu.make_async_remote_copy(
            src_ref=dst,
            dst_ref=dst,
            send_sem=send_sem.at[kind, landed],
            recv_sem=recv_sem.at[kind, landed],
            device_id=partner,
            device_id_type=MESH,
        ).wait_recv()

    def to_partner(kind, src, dst):
        return pltpu.make_async_remote_copy(
            src_ref=src,
            dst_ref=dst,
            send_sem=tsend_sem.at[kind],
            recv_sem=trecv_sem.at[kind],
            device_id=partner,
            device_id_type=MESH,
        )

    def spread_out(kind, peer, dst, offsets):
        for d in offsets:
            send(kind, peer(d), dst.at[0], dst.at[slot(-d)], slot(d), slot(-d))

    def forward(kind, peer, dst, place):
        if not tree:
            return
        for back, on in ((-2, 1), (2, -1)):
            arrived(kind, dst.at[slot(back)], slot(back))
            to = slot(back - on)
            send(kind, peer(on), dst.at[slot(back)], dst.at[to], slot(on - back), to)
        way = 1 - 2 * lax.rem(place, 2)
        middle = lax.div(7 + way, 2)
        send(kind, peer(2 * way), dst.at[middle], dst.at[slot(4)], slot(4), slot(4))

    def rest_arrived(kind, dst, offsets):
        for d in offsets:
            arrived(kind, dst.at[slot(d)], slot(d))

    beyond = [1, -1, 3, -3, 4] if tree else near

    sends = []

    def go(copy):
        copy.start()
        sends.append(copy)
        return copy

    loads = {
        name: pltpu.make_async_copy(src, local[name], load_sem.at[i])
        for i, (name, src) in enumerate(zip(names, hbm))
    }
    later = names.index("din")
    for name in names[:later]:
        loads[name].start()
    barrier = pltpu.get_barrier_semaphore()
    pl.semaphore_signal(barrier, inc=1, device_id=partner, device_id_type=MESH)
    for d in range(1, side):
        for device in (line_peer(d), cross_peer(d)):
            pl.semaphore_signal(barrier, inc=1, device_id=device, device_id_type=MESH)
    bulk = names.index("gs")
    for name in names[later:bulk]:
        loads[name].start()

    def loaded(*wanted):
        for name in wanted:
            loads[name].wait()

    groups, states = local["rate"].shape
    members = local["skip"].shape[1]
    channels = groups * members
    pair = 2 * states
    drive_v[...] = jnp.zeros_like(drive_v)
    omap_v[...] = jnp.zeros_like(omap_v)
    loaded("rate", "freq", "step", "imap", "omap", "skip")
    rate, freq = local["rate"][...], local["freq"][...]
    eye = iota((groups, groups), 0) == iota((groups, groups), 1)
    step = jnp.exp(jnp.sum(jnp.where(eye, local["step"][...], 0.0), axis=1, keepdims=True))
    magnitude = jnp.exp(-rate * step)
    angle = freq * step
    decay_re, decay_im = magnitude * jnp.cos(angle), magnitude * jnp.sin(angle)
    denominator = rate * rate + freq * freq
    factor_re = ((decay_re - 1.0) * -rate + decay_im * freq) / denominator
    factor_im = (decay_im * -rate - (decay_re - 1.0) * freq) / denominator
    same = jnp.concatenate([decay_re, decay_re], axis=1)
    cross = jnp.concatenate([-decay_im, decay_im], axis=1)
    for g in range(groups):
        fr, fi = factor_re[g : g + 1], factor_im[g : g + 1]
        m0, m1 = local["imap"][0, g], local["imap"][1, g]
        drive = jnp.concatenate([fr * m0 - fi * m1, fr * m1 + fi * m0], axis=1)
        out = jnp.concatenate([local["omap"][0, g], -local["omap"][1, g]], axis=1)
        odd = g % 2
        at, lanes_at = pl.ds(odd * members, members), pl.ds(odd * pair, pair)
        drive_v[0, g // 2, at, lanes_at], drive_v[1, g // 2, at, lanes_at] = halves(drive)
        omap_v[g // 2, at, lanes_at] = out.astype(bf16)
    tile = jnp.where(
        iota((members, channels), 0)
        == iota((members, channels), 1)
        - jnp.floor((iota((members, channels), 1) + 0.5) / members) * members,
        1.0,
        0.0,
    )
    skip = jnp.dot(local["skip"][...], tile, preferred_element_type=f32, precision=highest)
    in_group = jnp.floor((iota((groups, channels), 1) + 0.5) / members) == iota(
        (groups, channels), 0
    )
    skip = jnp.sum(jnp.where(in_group, skip, 0.0), axis=0, keepdims=True)
    loaded("x", "win")
    for name in names[bulk:]:
        loads[name].start()
    projected = dot(x_ref[...], local["win"][...]).astype(bf16)
    pushed = []
    for j in range(groups // 2):
        inputs = projected[:, 2 * j * members : 2 * (j + 1) * members]
        pushed.append(dot(inputs, drive_v[0, j]) + dot(inputs, drive_v[1, j]))
    loaded("state")
    response = skip * projected.astype(f32)
    states_now = []
    for g in range(groups):
        old = jnp.concatenate(
            [
                local["state"][pl.ds(g, rows, stride=groups)],
                local["state"][pl.ds(rows * groups + g, rows, stride=groups)],
            ],
            axis=1,
        )
        turned = jnp.concatenate([old[:, states:], old[:, :states]], axis=1)
        new = same[g : g + 1] * old + cross[g : g + 1] * turned
        new += pushed[g // 2][:, g % 2 * pair : (g % 2 + 1) * pair]
        new_ref[pl.ds(g, rows, stride=groups)] = new[:, :states]
        new_ref[pl.ds(rows * groups + g, rows, stride=groups)] = new[:, states:]
        states_now.append(new.astype(bf16))
    response += jnp.concatenate(
        [
            dot_t(jnp.concatenate(states_now[2 * j : 2 * j + 2], axis=1), omap_v[j])
            for j in range(groups // 2)
        ],
        axis=1,
    )
    act_send[...] = jax.nn.gelu(response).astype(bf16)

    pl.semaphore_wait(barrier, 2 * side - 1)
    act_copy = go(to_partner(0, act_send, act_all.at[core]))
    act_all[core] = act_send[...]
    loaded("din", "dout")
    din_all[0] = din_ref[...]
    dout_all[0] = dout_ref[...]
    spread_out(DIN, cross_peer, din_all, near)
    spread_out(DOUT, cross_peer, dout_all, near)

    lanes = meta.shape[2]
    loaded("ids", "scores")
    ids, scores = local["ids"][...].astype(f32), local["scores"][...]
    scores = scores / jnp.sum(scores, axis=0, keepdims=True) * route_scale
    eye = iota((rows, rows), 0) == iota((rows, rows), 1)
    lane = iota((rows, lanes), 1)
    hits = jnp.zeros((rows, lanes), f32)
    share = jnp.zeros((rows, lanes), f32)
    for k in range(ids.shape[0]):
        name = jnp.sum(jnp.where(eye, ids[k : k + 1], 0.0), axis=1, keepdims=True)
        score = jnp.sum(jnp.where(eye, scores[k : k + 1], 0.0), axis=1, keepdims=True)
        hits += jnp.where(lane == name, 1.0, 0.0)
        share += jnp.where(lane == name + experts, score, 0.0)
    earlier = jnp.where(iota((rows, rows), 1) < iota((rows, rows), 0), 1.0, 0.0)
    ranks = dot(earlier.astype(bf16), hits.astype(bf16))
    codes = jnp.where(hits > 0.5, ranks, -1.0)
    meta[0] = jnp.where(lane < experts, codes, share).astype(bf16)
    spread_out(META, line_peer, meta, order)

    loaded("glu", "mix", "gain", "shift")
    glu_v, mix_v = local["glu"], local["mix"]
    act_copy.wait_recv()
    a0, a1 = act_all[0], act_all[1]
    gate = dot(a0, glu_v[:channels]) + dot(a1, glu_v[channels:])
    g0 = (a0.astype(f32) * jax.nn.sigmoid(gate[:, :channels])).astype(bf16)
    g1 = (a1.astype(f32) * jax.nn.sigmoid(gate[:, channels:])).astype(bf16)
    mixed = (dot(g0, mix_v[:channels]) + dot(g1, mix_v[channels:])).astype(bf16)
    values = residual_alpha * x_ref[...].astype(f32) + mixed.astype(f32)
    mean = jnp.mean(values, axis=1, keepdims=True)
    centred = values - mean
    variance = jnp.mean(centred * centred, axis=1, keepdims=True)
    normed = (centred * lax.rsqrt(variance + norm_eps) * local["gain"][...] + local["shift"][...]).astype(
        bf16
    )
    left, right = normed[:, :half], normed[:, half:]
    first = core == 0
    own = jnp.where(first, left, right)
    oth = jnp.where(first, right, left)
    own_all[0] = own
    oth_all[0] = oth
    spread_out(OWN, line_peer, own_all, near)

    rest_arrived(META, meta, order)

    def steps(index):
        odd = index - 2.0 * jnp.floor((index + 0.5) / 2.0)
        ahead = jnp.floor((index + 1.5) / 2.0)
        return jnp.where(odd > 0.5, ahead, -ahead)

    def parts_of(index):
        part = jnp.floor((index + 0.5) / part_rows)
        index = index - part * part_rows
        cross_slot = jnp.floor((index + 0.5) / slots)
        index = index - cross_slot * slots
        member = jnp.floor((index + 0.5) / cap)
        return cross_slot, part * group + member, index - member * cap

    cross_slot, line_slot, at_rank = parts_of(iota((1, every), 1))
    pf, qf, cf = p.astype(f32), q.astype(f32), core.astype(f32)
    at_q = qf + steps(cross_slot)
    at_q = at_q - side * jnp.floor((at_q + 0.5) / side)
    expert = (1.0 - cf) * (at_q * side + pf) + cf * (pf * side + at_q)
    at_lane = iota((lanes, every), 0)
    every_meta = meta[...].reshape(line_rows, lanes)
    codes = dot(every_meta, jnp.where(at_lane == expert, 1.0, 0.0).astype(bf16))
    shares = dot(every_meta, jnp.where(at_lane == expert + experts, 1.0, 0.0).astype(bf16))
    block = jnp.floor((iota((line_rows, 1), 0) + 0.5) / rows)
    chosen = jnp.where((codes == at_rank) & (block == line_slot), 1.0, 0.0)
    weighted = (chosen * shares).astype(bf16)
    part_tokens = group * rows
    for h in range(2):
        tokens = slice(h * part_tokens, (h + 1) * part_tokens)
        lanes_at = slice(h * part_rows, (h + 1) * part_rows)
        mix_w[h] = weighted[tokens, lanes_at]
        pick_v[h] = chosen[tokens, lanes_at].T.astype(bf16)

    forward(OWN, line_peer, own_all, p)

    loaded("gs", "us", "ds")
    gs_v, us_v, ds_v = local["gs"], local["us"], local["ds"]
    hidden = (jax.nn.silu(dot(normed, gs_v[...])) * dot(normed, us_v[...])).astype(bf16)
    base = core * half
    other = (1 - core) * half
    sh_send[...] = dot(hidden, ds_v[:, pl.ds(pl.multiple_of(other, 128), half)]).astype(bf16)
    shared_copy = go(to_partner(4 + 2 * side, sh_send, sh_recv))
    shared_own = dot(hidden, ds_v[:, pl.ds(pl.multiple_of(base, 128), half)]).astype(bf16)

    for h in range(2):
        first_ones = [1, -1] if h == 0 else [3, -3, 4]
        if not tree:
            first_ones = [d for d in near if slot(d) // group == h]
        rest_arrived(OWN, own_all, first_ones)
        tokens = own_all[h * group : (h + 1) * group].reshape(part_tokens, half)
        x_send[h] = dot(pick_v[h], tokens).astype(bf16).reshape(side, slots, half)
        for d in order:
            place = slot(d)
            send(
                XS + h, cross_peer(d), x_send.at[h, place], x_recv.at[h, slot(-d)], place, slot(-d)
            )
        x_recv[h, 0] = x_send[h, 0]

    mine = parts_of(iota((every, 1), 0))
    theirs = parts_of(iota((1, every), 1))
    swap = jnp.where(
        (mine[0] == theirs[1]) & (mine[1] == theirs[0]) & (mine[2] == theirs[2]), 1.0, 0.0
    ).astype(bf16)

    def hand_over(h, k):
        return to_partner(4 + h * side + k, x_recv.at[h, k], x_oth.at[h, k])

    for h in range(2):
        go(hand_over(h, 0))
        for d in order:
            arrived(XS + h, x_recv.at[h, slot(d)], slot(d))
            go(hand_over(h, slot(d)))
    spread_out(OTH, line_peer, oth_all, near)
    forward(DIN, cross_peer, din_all, q)
    forward(DOUT, cross_peer, dout_all, q)
    loaded("ge", "ue", "de")
    ge_v, ue_v, de_v = local["ge"], local["ue"], local["de"]
    tok = x_recv[...].reshape(every, half)
    at = pl.ds(pl.multiple_of(base, 128), half)
    gate, up = dot(tok, ge_v[at]), dot(tok, ue_v[at])
    for h in range(2):
        for k in range(side):
            hand_over(h, k).wait_recv()
    tok = dot(swap, x_oth[...].reshape(every, half)).astype(bf16)
    at = pl.ds(pl.multiple_of(other, 128), half)
    gate += dot(tok, ge_v[at])
    up += dot(tok, ue_v[at])
    hidden = (jax.nn.silu(gate) * up).astype(bf16)
    down_own = de_v[:, pl.ds(pl.multiple_of(base, 128), half)]
    down_other = de_v[:, pl.ds(pl.multiple_of(other, 128), half)]
    for_partner = dot(swap, hidden).astype(bf16)
    for h in (1, 0):
        at = slice(h * part_rows, (h + 1) * part_rows)
        y_send[h] = dot(for_partner[at], down_other).astype(bf16)
        go(to_partner(2 if h else 1, y_send.at[h], y_oth.at[h]))
    result = dot(hidden, down_own)
    for h in (1, 0):
        to_partner(2 if h else 1, y_send.at[h], y_oth.at[h]).wait_recv()
        at = slice(h * part_rows, (h + 1) * part_rows)
        total = result[at] + y_oth[h].astype(f32)
        r_send[h] = total.astype(bf16).reshape(side, slots, half)
        for d in order:
            place = slot(d)
            send(
                RS + h, cross_peer(d), r_send.at[h, place], r_recv.at[h, slot(-d)], place, slot(-d)
            )
        r_recv[h, 0] = r_send[h, 0]
        if h:
            forward(OTH, line_peer, oth_all, p)

    rest_arrived(OTH, oth_all, beyond)
    rest_arrived(DIN, din_all, beyond)
    rest_arrived(DOUT, dout_all, beyond)
    units = side * din_ref.shape[0]
    din = din_all[...].reshape(units, width)
    din_left, din_right = din[:, :half], din[:, half:]
    din_own = jnp.where(first, din_left, din_right)
    din_oth = jnp.where(first, din_right, din_left)
    loaded("bgate")
    bgate = local["bgate"][...].astype(f32)
    bgate = jnp.concatenate([bgate[k : k + 1] for k in range(bgate.shape[0])], axis=1)
    bgate = jnp.broadcast_to(bgate, (8, width)).astype(bf16)
    b_own = jnp.where(first, bgate[:, :half], bgate[:, half:])
    b_oth = jnp.where(first, bgate[:, half:], bgate[:, :half])
    oth_tok = oth_all[...].reshape(line_rows, half)
    own_tok = own_all[...].reshape(line_rows, half)
    before = dot_t(oth_tok, din_oth) + dot_t(own_tok, din_own)
    gate = dot_t(oth_tok, b_oth) + dot_t(own_tok, b_own)
    dense_hidden = jax.nn.gelu(before).astype(bf16)
    branch = jax.nn.sigmoid(gate[:, :1])
    dense_v[...] = branch * dot(dense_hidden, dout_all[...].reshape(units, half))

    def send_sum(on, src, dst, sent, landed):
        send(SS, line_peer(on), src, dst, sent, landed)

    way = 1 - 2 * lax.rem(p, 2)

    def merge(k, d):
        arrived(SS, relay.at[k], slot(3 - 6 * k))
        mine = s_send[slot(d)].astype(f32) + relay[k].astype(f32)
        mine += jnp.where(d * way < 0, relay[2].astype(f32), 0.0)
        merged[k] = mine.astype(bf16)
        send_sum(d, merged.at[k], s_recv.at[slot(-d)], slot(d), slot(-d))

    for h in (1, 0):
        for d in order:
            arrived(RS + h, r_recv.at[h, slot(d)], slot(d))
        tokens = slice(h * part_tokens, (h + 1) * part_tokens)
        part = dot(mix_w[h], r_recv[h].reshape(part_rows, half)) + dense_v[tokens]
        s_send[h * group : (h + 1) * group] = part.astype(bf16).reshape(group, rows, half)
        if not tree:
            for d in order:
                if slot(d) // group == h:
                    send_sum(d, s_send.at[slot(d)], s_recv.at[slot(-d)], slot(d), slot(-d))
        elif h:
            send_sum(-2 * way, s_send.at[slot(4)], relay.at[2], slot(4), slot(4))
            send_sum(-1, s_send.at[slot(-3)], relay.at[0], slot(-3), slot(3))
            send_sum(1, s_send.at[slot(3)], relay.at[1], slot(3), slot(-3))
            arrived(SS, relay.at[2], slot(4))
            merge(0, -2)
        else:
            merge(1, 2)
            for d in (1, -1):
                send_sum(d, s_send.at[slot(d)], s_recv.at[slot(-d)], slot(d), slot(-d))

    shared_copy.wait_recv()
    shared = (shared_own.astype(f32) + sh_recv[...].astype(f32)).astype(bf16).astype(f32)
    skip = residual_alpha * own.astype(f32) + shared
    total = skip + s_send[0].astype(f32)
    for d in near:
        arrived(SS, s_recv.at[slot(d)], slot(d))
        total += s_recv[slot(d)].astype(f32)
    loaded("fgain", "fshift")
    row_sum = jnp.sum(total, axis=1, keepdims=True)
    row_squares = jnp.sum(total * total, axis=1, keepdims=True)
    st_send[...] = jnp.where(iota(st_send.shape, 1) < 0.5, row_sum, row_squares)
    st_copy = go(to_partner(3, st_send, st_recv))
    st_copy.wait_recv()
    mean = (row_sum + st_recv[:, 0:1]) / width
    variance = (row_squares + st_recv[:, 1:2]) / width - mean * mean
    scale = lax.rsqrt(variance + norm_eps)
    out = (total - mean) * scale * local["fgain"][...] + local["fshift"][...]
    out_ref[...] = out.astype(bf16)
    for copy in sends:
        copy.wait_send()


def layer(side, cap, experts, args):
    names = tuple(args)
    rows, width = args["x"].shape
    groups, states = args["rate"].shape
    channels = args["win"].shape[1]
    half = width // 2
    group = side // 2
    slots = group * cap
    part_rows = side * slots
    every = 2 * part_rows
    lanes = -(-2 * experts // 128) * 128
    din, dout = args["din"], args["dout"]
    kinds = 10
    V = pltpu.VMEM
    return pl.pallas_call(
        functools.partial(layer_kernel, side, cap, experts, names),
        out_shape=(
            pltpu.VMEM((rows, half), bf16),
            pltpu.VMEM(args["state"].shape, f32),
        ),
        in_specs=[pl.BlockSpec(memory_space=pl.ANY)] * len(names),
        out_specs=(pl.BlockSpec(memory_space=pltpu.VMEM),) * 2,
        scratch_shapes=[V(a.shape, a.dtype) for a in args.values()]
        + [
            V((2, groups // 2, 2 * channels // groups, 4 * states), bf16),
            V((groups // 2, 2 * channels // groups, 4 * states), bf16),
            V((rows, channels), bf16),
            V((2, rows, channels), bf16),
            V((side, rows, lanes), bf16),
            V((side, *din.shape), bf16),
            V((side, *dout.shape), bf16),
            V((side, rows, half), bf16),
            V((side, rows, half), bf16),
            V((2, side, slots, half), bf16),
            V((2, side, slots, half), bf16),
            V((2, side, slots, half), bf16),
            V((2, part_rows, half), bf16),
            V((2, part_rows, half), bf16),
            V((2, side, slots, half), bf16),
            V((2, side, slots, half), bf16),
            V((side, rows, half), bf16),
            V((side, rows, half), bf16),
            V((3, rows, half), bf16),
            V((2, rows, half), bf16),
            V((rows, half), bf16),
            V((rows, half), bf16),
            V((rows, 128), f32),
            V((rows, 128), f32),
            V((2, part_rows, group * rows), bf16),
            V((2, group * rows, part_rows), bf16),
            V((side * rows, half), f32),
            pltpu.SemaphoreType.DMA((len(names),)),
            pltpu.SemaphoreType.DMA((kinds, side)),
            pltpu.SemaphoreType.DMA((kinds, side)),
            pltpu.SemaphoreType.DMA((5 + 2 * side,)),
            pltpu.SemaphoreType.DMA((5 + 2 * side,)),
        ],
        compiler_params=pltpu.CompilerParams(
            collective_id=0, has_side_effects=True, vmem_limit_bytes=VMEM_BYTES
        ),
        name="layer",
    )(*args.values())


def write_out(*refs):
    count = (len(refs) - 1) // 2
    copies = [
        pltpu.make_async_copy(refs[i], refs[count + i], refs[-1].at[i]) for i in range(count)
    ]
    for copy in copies:
        copy.start()
    for copy in copies:
        copy.wait()


def to_memory(*arrays):
    return pl.pallas_call(
        write_out,
        out_shape=tuple(jax.ShapeDtypeStruct(a.shape, a.dtype) for a in arrays),
        in_specs=[pl.BlockSpec(memory_space=pltpu.VMEM)] * len(arrays),
        out_specs=(pl.BlockSpec(memory_space=pltpu.HBM),) * len(arrays),
        scratch_shapes=[pltpu.SemaphoreType.DMA((len(arrays),))],
        name="write_out",
    )(*(pltpu.with_memory_space_constraint(a, pltpu.VMEM) for a in arrays))


def body(
    layer_input,
    ssm_state,
    w_input,
    decay_rate,
    frequency,
    step_log,
    input_map,
    output_map,
    skip_gain,
    glu_weight,
    mix_out,
    norm_gain,
    norm_shift,
    route_ids,
    route_weights,
    gate_expert,
    up_expert,
    down_expert,
    gate_shared,
    up_shared,
    down_shared,
    dense_in,
    dense_out,
    branch_gate,
    final_gain,
    final_shift,
):
    count_ep = lax.axis_size("ep")
    count_tp = lax.axis_size("tp")
    seq_rows, width = layer_input.shape
    top_k = route_ids.shape[1]
    experts = gate_expert.shape[0] * count_ep
    cap = count_tp * max(1, min(seq_rows // count_tp, seq_rows * top_k // experts))
    side = math.isqrt(count_ep)
    layer_output, new_state = layer(
        side,
        cap,
        experts,
        dict(
            ids=route_ids.T,
            scores=route_weights.T,
            rate=decay_rate,
            freq=frequency,
            step=step_log[None],
            imap=input_map.transpose(0, 1, 3, 2),
            omap=output_map,
            skip=skip_gain,
            x=layer_input,
            win=w_input,
            state=ssm_state.reshape(-1, ssm_state.shape[3]),
            din=dense_in,
            dout=dense_out,
            glu=glu_weight,
            mix=mix_out,
            gain=norm_gain[None],
            shift=norm_shift[None],
            gs=gate_shared,
            us=up_shared,
            ds=down_shared,
            ge=gate_expert[0],
            ue=up_expert[0],
            de=down_expert[0],
            bgate=branch_gate.reshape(-1, 128),
            fgain=final_gain[None],
            fshift=final_shift[None],
        ),
    )
    layer_output, new_state = to_memory(layer_output, new_state)
    new_state = new_state.reshape(ssm_state.shape)
    return (layer_output, new_state)


def solution(mesh):
    placed = (
        P(("grp", "ep"), None),
        P(None, ("grp", "ep"), "tp", None),
        P(None, "tp"),
        P("tp", None),
        P("tp", None),
        P("tp"),
        P(None, "tp", None, None),
        P(None, "tp", None, None),
        P("tp", None),
        P(),
        P(),
        P(),
        P(),
        P(("grp", "ep"), None),
        P(("grp", "ep"), None),
        P("ep", None, "tp"),
        P("ep", None, "tp"),
        P("ep", "tp", None),
        P(None, "tp"),
        P(None, "tp"),
        P("tp", None),
        P("ep", None),
        P("ep", "tp"),
        P(),
        P("tp"),
        P("tp"),
    )
    return jax.shard_map(
        body,
        mesh=mesh,
        in_specs=placed,
        out_specs=(P(("grp", "ep"), "tp"), P(None, ("grp", "ep"), "tp", None)),
        check_vma=False,
    )
```

```python
import functools
import math

import jax
import jax.numpy as jnp
from jax import lax
from jax.experimental import pallas as pl
from jax.experimental.pallas import tpu as pltpu
from jax.sharding import PartitionSpec as P

residual_alpha = 1.681792830507429
route_scale = 2.5
norm_eps = 1e-05
highest = lax.Precision.HIGHEST
MESH = pl.DeviceIdType.MESH
f32 = jnp.float32
bf16 = jnp.bfloat16
VMEM_BYTES = 64 * 1024 * 1024 - 1024 * 1024


def dot(a, b):
    return jnp.dot(a, b, preferred_element_type=f32)


def dot_t(a, b):
    return lax.dot_general(a, b, (((1,), (1,)), ((), ())), preferred_element_type=f32)


def iota(shape, dim):
    return lax.broadcasted_iota(jnp.int32, shape, dim).astype(f32)


def halves(a):
    high = a.astype(bf16)
    return high, (a - high.astype(f32)).astype(bf16)


def layer_kernel(side, cap, experts, names, *refs):
    count = len(names)
    hbm = refs[:count]
    out_ref, new_ref = refs[count : count + 2]
    local = dict(zip(names, refs[count + 2 :]))
    rest = refs[2 * count + 2 :]
    layer_steps(side, cap, experts, names, hbm, local, out_ref, new_ref, *rest)


def layer_steps(
    side,
    cap,
    experts,
    names,
    hbm,
    local,
    out_ref,
    new_ref,
    drive_v,
    omap_v,
    act_send,
    act_all,
    meta,
    din_all,
    dout_all,
    own_all,
    oth_all,
    x_send,
    x_recv,
    x_oth,
    y_send,
    y_oth,
    r_send,
    r_recv,
    s_send,
    s_recv,
    relay,
    merged,
    sh_send,
    sh_recv,
    st_send,
    st_recv,
    pick_v,
    mix_w,
    dense_v,
    load_sem,
    send_sem,
    recv_sem,
    tsend_sem,
    trecv_sem,
):
    x_ref, din_ref, dout_ref = local["x"], local["din"], local["dout"]
    rows, width = x_ref.shape
    half = width // 2
    line_rows = side * rows
    group = side // 2
    slots = group * cap
    part_rows = side * slots
    every = 2 * part_rows
    core = lax.axis_index("tp")
    chip = lax.axis_index("ep")
    row, col = lax.div(chip, side), lax.rem(chip, side)
    p = (1 - core) * col + core * row
    q = (1 - core) * row + core * col

    def chip_at(pp, qq):
        return (1 - core) * (qq * side + pp) + core * (pp * side + qq)

    def slot(d):
        d = (d + side - 1) % side
        d = d + 1 - side if d + 1 > side // 2 else d + 1
        return 2 * d - 1 if d > 0 else -2 * d

    def line_peer(d):
        return {"ep": chip_at(lax.rem(p + d + side, side), q), "tp": core}

    def cross_peer(d):
        return {"ep": chip_at(p, lax.rem(q + d + side, side)), "tp": core}

    partner = {"ep": chip, "tp": 1 - core}
    tree = side == 8
    near = [d for d in (2, -2, 1, -1) if tree] or list(range(1, side))
    order = sorted(range(1, side), key=lambda d: -min(d, side - d))
    if tree:
        order = [4, 3, -3, 2, -2, 1, -1]

    META, DIN, DOUT, OTH, OWN, XS, RS, SS = 0, 1, 2, 3, 4, 5, 7, 9

    def send(kind, device, src, dst, sent, landed):
        go(
            pltpu.make_async_remote_copy(
                src_ref=src,
                dst_ref=dst,
                send_sem=send_sem.at[kind, sent],
                recv_sem=recv_sem.at[kind, landed],
                device_id=device,
                device_id_type=MESH,
            )
        )

    def arrived(kind, dst, landed):
        pltpu.make_async_remote_copy(
            src_ref=dst,
            dst_ref=dst,
            send_sem=send_sem.at[kind, landed],
            recv_sem=recv_sem.at[kind, landed],
            device_id=partner,
            device_id_type=MESH,
        ).wait_recv()

    def to_partner(kind, src, dst):
        return pltpu.make_async_remote_copy(
            src_ref=src,
            dst_ref=dst,
            send_sem=tsend_sem.at[kind],
            recv_sem=trecv_sem.at[kind],
            device_id=partner,
            device_id_type=MESH,
        )

    def spread_out(kind, peer, dst, offsets):
        for d in offsets:
            send(kind, peer(d), dst.at[0], dst.at[slot(-d)], slot(d), slot(-d))

    def forward(kind, peer, dst, place):
        if not tree:
            return
        for back, on in ((-2, 1), (2, -1)):
            arrived(kind, dst.at[slot(back)], slot(back))
            to = slot(back - on)
            send(kind, peer(on), dst.at[slot(back)], dst.at[to], slot(on - back), to)
        way = 1 - 2 * lax.rem(place, 2)
        middle = lax.div(7 + way, 2)
        send(kind, peer(2 * way), dst.at[middle], dst.at[slot(4)], slot(4), slot(4))

    def rest_arrived(kind, dst, offsets):
        for d in offsets:
            arrived(kind, dst.at[slot(d)], slot(d))

    beyond = [1, -1, 3, -3, 4] if tree else near

    sends = []

    def go(copy):
        copy.start()
        sends.append(copy)
        return copy

    loads = {
        name: pltpu.make_async_copy(src, local[name], load_sem.at[i])
        for i, (name, src) in enumerate(zip(names, hbm))
    }
    later = names.index("din")
    for name in names[:later]:
        loads[name].start()
    barrier = pltpu.get_barrier_semaphore()
    pl.semaphore_signal(barrier, inc=1, device_id=partner, device_id_type=MESH)
    for d in range(1, side):
        for device in (line_peer(d), cross_peer(d)):
            pl.semaphore_signal(barrier, inc=1, device_id=device, device_id_type=MESH)
    bulk = names.index("gs")
    for name in names[later:bulk]:
        loads[name].start()

    def loaded(*wanted):
        for name in wanted:
            loads[name].wait()

    groups, states = local["rate"].shape
    members = local["skip"].shape[1]
    channels = groups * members
    pair = 2 * states
    drive_v[...] = jnp.zeros_like(drive_v)
    omap_v[...] = jnp.zeros_like(omap_v)
    loaded("rate", "freq", "step", "imap", "omap", "skip")
    rate, freq = local["rate"][...], local["freq"][...]
    eye = iota((groups, groups), 0) == iota((groups, groups), 1)
    step = jnp.exp(jnp.sum(jnp.where(eye, local["step"][...], 0.0), axis=1, keepdims=True))
    magnitude = jnp.exp(-rate * step)
    angle = freq * step
    decay_re, decay_im = magnitude * jnp.cos(angle), magnitude * jnp.sin(angle)
    denominator = rate * rate + freq * freq
    factor_re = ((decay_re - 1.0) * -rate + decay_im * freq) / denominator
    factor_im = (decay_im * -rate - (decay_re - 1.0) * freq) / denominator
    same = jnp.concatenate([decay_re, decay_re], axis=1)
    cross = jnp.concatenate([-decay_im, decay_im], axis=1)
    for g in range(groups):
        fr, fi = factor_re[g : g + 1], factor_im[g : g + 1]
        m0, m1 = local["imap"][0, g], local["imap"][1, g]
        drive = jnp.concatenate([fr * m0 - fi * m1, fr * m1 + fi * m0], axis=1)
        out = jnp.concatenate([local["omap"][0, g], -local["omap"][1, g]], axis=1)
        odd = g % 2
        at, lanes_at = pl.ds(odd * members, members), pl.ds(odd * pair, pair)
        drive_v[0, g // 2, at, lanes_at], drive_v[1, g // 2, at, lanes_at] = halves(drive)
        omap_v[g // 2, at, lanes_at] = out.astype(bf16)
    tile = jnp.where(
        iota((members, channels), 0)
        == iota((members, channels), 1)
        - jnp.floor((iota((members, channels), 1) + 0.5) / members) * members,
        1.0,
        0.0,
    )
    skip = jnp.dot(local["skip"][...], tile, preferred_element_type=f32, precision=highest)
    in_group = jnp.floor((iota((groups, channels), 1) + 0.5) / members) == iota(
        (groups, channels), 0
    )
    skip = jnp.sum(jnp.where(in_group, skip, 0.0), axis=0, keepdims=True)
    loaded("x", "win")
    for name in names[bulk:]:
        loads[name].start()
    projected = dot(x_ref[...], local["win"][...]).astype(bf16)
    pushed = []
    for j in range(groups // 2):
        inputs = projected[:, 2 * j * members : 2 * (j + 1) * members]
        pushed.append(dot(inputs, drive_v[0, j]) + dot(inputs, drive_v[1, j]))
    loaded("state")
    response = skip * projected.astype(f32)
    states_now = []
    for g in range(groups):
        old = jnp.concatenate(
            [
                local["state"][pl.ds(g, rows, stride=groups)],
                local["state"][pl.ds(rows * groups + g, rows, stride=groups)],
            ],
            axis=1,
        )
        turned = jnp.concatenate([old[:, states:], old[:, :states]], axis=1)
        new = same[g : g + 1] * old + cross[g : g + 1] * turned
        new += pushed[g // 2][:, g % 2 * pair : (g % 2 + 1) * pair]
        new_ref[pl.ds(g, rows, stride=groups)] = new[:, :states]
        new_ref[pl.ds(rows * groups + g, rows, stride=groups)] = new[:, states:]
        states_now.append(new.astype(bf16))
    response += jnp.concatenate(
        [
            dot_t(jnp.concatenate(states_now[2 * j : 2 * j + 2], axis=1), omap_v[j])
            for j in range(groups // 2)
        ],
        axis=1,
    )
    act_send[...] = jax.nn.gelu(response).astype(bf16)

    pl.semaphore_wait(barrier, 2 * side - 1)
    act_copy = go(to_partner(0, act_send, act_all.at[core]))
    act_all[core] = act_send[...]
    loaded("din", "dout")
    din_all[0] = din_ref[...]
    dout_all[0] = dout_ref[...]
    spread_out(DIN, cross_peer, din_all, near)
    spread_out(DOUT, cross_peer, dout_all, near)

    lanes = meta.shape[2]
    loaded("ids", "scores")
    ids, scores = local["ids"][...].astype(f32), local["scores"][...]
    scores = scores / jnp.sum(scores, axis=0, keepdims=True) * route_scale
    eye = iota((rows, rows), 0) == iota((rows, rows), 1)
    lane = iota((rows, lanes), 1)
    hits = jnp.zeros((rows, lanes), f32)
    share = jnp.zeros((rows, lanes), f32)
    for k in range(ids.shape[0]):
        name = jnp.sum(jnp.where(eye, ids[k : k + 1], 0.0), axis=1, keepdims=True)
        score = jnp.sum(jnp.where(eye, scores[k : k + 1], 0.0), axis=1, keepdims=True)
        hits += jnp.where(lane == name, 1.0, 0.0)
        share += jnp.where(lane == name + experts, score, 0.0)
    earlier = jnp.where(iota((rows, rows), 1) < iota((rows, rows), 0), 1.0, 0.0)
    ranks = dot(earlier.astype(bf16), hits.astype(bf16))
    codes = jnp.where(hits > 0.5, ranks, -1.0)
    meta[0] = jnp.where(lane < experts, codes, share).astype(bf16)
    spread_out(META, line_peer, meta, order)

    loaded("glu", "mix", "gain", "shift")
    glu_v, mix_v = local["glu"], local["mix"]
    act_copy.wait_recv()
    a0, a1 = act_all[0], act_all[1]
    gate = dot(a0, glu_v[:channels]) + dot(a1, glu_v[channels:])
    g0 = (a0.astype(f32) * jax.nn.sigmoid(gate[:, :channels])).astype(bf16)
    g1 = (a1.astype(f32) * jax.nn.sigmoid(gate[:, channels:])).astype(bf16)
    mixed = (dot(g0, mix_v[:channels]) + dot(g1, mix_v[channels:])).astype(bf16)
    values = residual_alpha * x_ref[...].astype(f32) + mixed.astype(f32)
    mean = jnp.mean(values, axis=1, keepdims=True)
    centred = values - mean
    variance = jnp.mean(centred * centred, axis=1, keepdims=True)
    normed = (centred * lax.rsqrt(variance + norm_eps) * local["gain"][...] + local["shift"][...]).astype(
        bf16
    )
    left, right = normed[:, :half], normed[:, half:]
    first = core == 0
    own = jnp.where(first, left, right)
    oth = jnp.where(first, right, left)
    own_all[0] = own
    oth_all[0] = oth
    spread_out(OWN, line_peer, own_all, near)

    rest_arrived(META, meta, order)

    def steps(index):
        odd = index - 2.0 * jnp.floor((index + 0.5) / 2.0)
        ahead = jnp.floor((index + 1.5) / 2.0)
        return jnp.where(odd > 0.5, ahead, -ahead)

    def parts_of(index):
        part = jnp.floor((index + 0.5) / part_rows)
        index = index - part * part_rows
        cross_slot = jnp.floor((index + 0.5) / slots)
        index = index - cross_slot * slots
        member = jnp.floor((index + 0.5) / cap)
        return cross_slot, part * group + member, index - member * cap

    cross_slot, line_slot, at_rank = parts_of(iota((1, every), 1))
    pf, qf, cf = p.astype(f32), q.astype(f32), core.astype(f32)
    at_q = qf + steps(cross_slot)
    at_q = at_q - side * jnp.floor((at_q + 0.5) / side)
    expert = (1.0 - cf) * (at_q * side + pf) + cf * (pf * side + at_q)
    at_lane = iota((lanes, every), 0)
    every_meta = meta[...].reshape(line_rows, lanes)
    codes = dot(every_meta, jnp.where(at_lane == expert, 1.0, 0.0).astype(bf16))
    shares = dot(every_meta, jnp.where(at_lane == expert + experts, 1.0, 0.0).astype(bf16))
    block = jnp.floor((iota((line_rows, 1), 0) + 0.5) / rows)
    chosen = jnp.where((codes == at_rank) & (block == line_slot), 1.0, 0.0)
    weighted = (chosen * shares).astype(bf16)
    part_tokens = group * rows
    for h in range(2):
        tokens = slice(h * part_tokens, (h + 1) * part_tokens)
        lanes_at = slice(h * part_rows, (h + 1) * part_rows)
        mix_w[h] = weighted[tokens, lanes_at]
        pick_v[h] = chosen[tokens, lanes_at].T.astype(bf16)

    forward(OWN, line_peer, own_all, p)

    loaded("gs", "us", "ds")
    gs_v, us_v, ds_v = local["gs"], local["us"], local["ds"]
    hidden = (jax.nn.silu(dot(normed, gs_v[...])) * dot(normed, us_v[...])).astype(bf16)
    base = core * half
    other = (1 - core) * half
    sh_send[...] = dot(hidden, ds_v[:, pl.ds(pl.multiple_of(other, 128), half)]).astype(bf16)
    shared_copy = go(to_partner(4 + 2 * side, sh_send, sh_recv))
    shared_own = dot(hidden, ds_v[:, pl.ds(pl.multiple_of(base, 128), half)]).astype(bf16)

    mine = parts_of(iota((every, 1), 0))
    theirs = parts_of(iota((1, every), 1))
    swap = jnp.where(
        (mine[0] == theirs[1]) & (mine[1] == theirs[0]) & (mine[2] == theirs[2]), 1.0, 0.0
    ).astype(bf16)

    for h in range(2):
        first_ones = [1, -1] if h == 0 else [3, -3, 4]
        if not tree:
            first_ones = [d for d in near if slot(d) // group == h]
        rest_arrived(OWN, own_all, first_ones)
        tokens = own_all[h * group : (h + 1) * group].reshape(part_tokens, half)
        x_send[h] = dot(pick_v[h], tokens).astype(bf16).reshape(side, slots, half)
        for d in order:
            place = slot(d)
            send(
                XS + h, cross_peer(d), x_send.at[h, place], x_recv.at[h, slot(-d)], place, slot(-d)
            )
        x_recv[h, 0] = x_send[h, 0]

    def hand_over(h, k):
        return to_partner(4 + h * side + k, x_recv.at[h, k], x_oth.at[h, k])

    for h in range(2):
        go(hand_over(h, 0))
        for d in order:
            arrived(XS + h, x_recv.at[h, slot(d)], slot(d))
            go(hand_over(h, slot(d)))
    spread_out(OTH, line_peer, oth_all, near)
    forward(DIN, cross_peer, din_all, q)
    forward(DOUT, cross_peer, dout_all, q)
    loaded("ge", "ue", "de")
    ge_v, ue_v, de_v = local["ge"], local["ue"], local["de"]
    tok = x_recv[...].reshape(every, half)
    at = pl.ds(pl.multiple_of(base, 128), half)
    gate, up = dot(tok, ge_v[at]), dot(tok, ue_v[at])
    for h in range(2):
        for k in range(side):
            hand_over(h, k).wait_recv()
    tok = dot(swap, x_oth[...].reshape(every, half)).astype(bf16)
    at = pl.ds(pl.multiple_of(other, 128), half)
    gate += dot(tok, ge_v[at])
    up += dot(tok, ue_v[at])
    hidden = (jax.nn.silu(gate) * up).astype(bf16)
    down_own = de_v[:, pl.ds(pl.multiple_of(base, 128), half)]
    down_other = de_v[:, pl.ds(pl.multiple_of(other, 128), half)]
    for_partner = dot(swap, hidden).astype(bf16)
    for h in (1, 0):
        at = slice(h * part_rows, (h + 1) * part_rows)
        y_send[h] = dot(for_partner[at], down_other).astype(bf16)
        go(to_partner(2 if h else 1, y_send.at[h], y_oth.at[h]))
    result = dot(hidden, down_own)
    for h in (1, 0):
        to_partner(2 if h else 1, y_send.at[h], y_oth.at[h]).wait_recv()
        at = slice(h * part_rows, (h + 1) * part_rows)
        total = result[at] + y_oth[h].astype(f32)
        r_send[h] = total.astype(bf16).reshape(side, slots, half)
        for d in order:
            place = slot(d)
            send(
                RS + h, cross_peer(d), r_send.at[h, place], r_recv.at[h, slot(-d)], place, slot(-d)
            )
        r_recv[h, 0] = r_send[h, 0]
        if h:
            forward(OTH, line_peer, oth_all, p)

    rest_arrived(OTH, oth_all, beyond)
    rest_arrived(DIN, din_all, beyond)
    rest_arrived(DOUT, dout_all, beyond)
    units = side * din_ref.shape[0]
    din = din_all[...].reshape(units, width)
    din_left, din_right = din[:, :half], din[:, half:]
    din_own = jnp.where(first, din_left, din_right)
    din_oth = jnp.where(first, din_right, din_left)
    loaded("bgate")
    bgate = local["bgate"][...].astype(f32)
    bgate = jnp.concatenate([bgate[k : k + 1] for k in range(bgate.shape[0])], axis=1)
    bgate = jnp.broadcast_to(bgate, (8, width)).astype(bf16)
    b_own = jnp.where(first, bgate[:, :half], bgate[:, half:])
    b_oth = jnp.where(first, bgate[:, half:], bgate[:, :half])
    oth_tok = oth_all[...].reshape(line_rows, half)
    own_tok = own_all[...].reshape(line_rows, half)
    before = dot_t(oth_tok, din_oth) + dot_t(own_tok, din_own)
    gate = dot_t(oth_tok, b_oth) + dot_t(own_tok, b_own)
    dense_hidden = jax.nn.gelu(before).astype(bf16)
    branch = jax.nn.sigmoid(gate[:, :1])
    dense_v[...] = branch * dot(dense_hidden, dout_all[...].reshape(units, half))

    def send_sum(on, src, dst, sent, landed):
        send(SS, line_peer(on), src, dst, sent, landed)

    way = 1 - 2 * lax.rem(p, 2)

    def merge(k, d):
        arrived(SS, relay.at[k], slot(3 - 6 * k))
        mine = s_send[slot(d)].astype(f32) + relay[k].astype(f32)
        mine += jnp.where(d * way < 0, relay[2].astype(f32), 0.0)
        merged[k] = mine.astype(bf16)
        send_sum(d, merged.at[k], s_recv.at[slot(-d)], slot(d), slot(-d))

    for h in (1, 0):
        for d in order:
            arrived(RS + h, r_recv.at[h, slot(d)], slot(d))
        tokens = slice(h * part_tokens, (h + 1) * part_tokens)
        part = dot(mix_w[h], r_recv[h].reshape(part_rows, half)) + dense_v[tokens]
        s_send[h * group : (h + 1) * group] = part.astype(bf16).reshape(group, rows, half)
        if not tree:
            for d in order:
                if slot(d) // group == h:
                    send_sum(d, s_send.at[slot(d)], s_recv.at[slot(-d)], slot(d), slot(-d))
        elif h:
            send_sum(-2 * way, s_send.at[slot(4)], relay.at[2], slot(4), slot(4))
            send_sum(-1, s_send.at[slot(-3)], relay.at[0], slot(-3), slot(3))
            send_sum(1, s_send.at[slot(3)], relay.at[1], slot(3), slot(-3))
            arrived(SS, relay.at[2], slot(4))
            merge(0, -2)
        else:
            merge(1, 2)
            for d in (1, -1):
                send_sum(d, s_send.at[slot(d)], s_recv.at[slot(-d)], slot(d), slot(-d))

    shared_copy.wait_recv()
    shared = (shared_own.astype(f32) + sh_recv[...].astype(f32)).astype(bf16).astype(f32)
    skip = residual_alpha * own.astype(f32) + shared
    total = skip + s_send[0].astype(f32)
    for d in near:
        arrived(SS, s_recv.at[slot(d)], slot(d))
        total += s_recv[slot(d)].astype(f32)
    loaded("fgain", "fshift")
    row_sum = jnp.sum(total, axis=1, keepdims=True)
    row_squares = jnp.sum(total * total, axis=1, keepdims=True)
    st_send[...] = jnp.where(iota(st_send.shape, 1) < 0.5, row_sum, row_squares)
    st_copy = go(to_partner(3, st_send, st_recv))
    st_copy.wait_recv()
    mean = (row_sum + st_recv[:, 0:1]) / width
    variance = (row_squares + st_recv[:, 1:2]) / width - mean * mean
    scale = lax.rsqrt(variance + norm_eps)
    out = (total - mean) * scale * local["fgain"][...] + local["fshift"][...]
    out_ref[...] = out.astype(bf16)
    for copy in sends:
        copy.wait_send()


def layer(side, cap, experts, args):
    names = tuple(args)
    rows, width = args["x"].shape
    groups, states = args["rate"].shape
    channels = args["win"].shape[1]
    half = width // 2
    group = side // 2
    slots = group * cap
    part_rows = side * slots
    every = 2 * part_rows
    lanes = -(-2 * experts // 128) * 128
    din, dout = args["din"], args["dout"]
    kinds = 10
    V = pltpu.VMEM
    return pl.pallas_call(
        functools.partial(layer_kernel, side, cap, experts, names),
        out_shape=(
            pltpu.VMEM((rows, half), bf16),
            pltpu.VMEM(args["state"].shape, f32),
        ),
        in_specs=[pl.BlockSpec(memory_space=pl.ANY)] * len(names),
        out_specs=(pl.BlockSpec(memory_space=pltpu.VMEM),) * 2,
        scratch_shapes=[V(a.shape, a.dtype) for a in args.values()]
        + [
            V((2, groups // 2, 2 * channels // groups, 4 * states), bf16),
            V((groups // 2, 2 * channels // groups, 4 * states), bf16),
            V((rows, channels), bf16),
            V((2, rows, channels), bf16),
            V((side, rows, lanes), bf16),
            V((side, *din.shape), bf16),
            V((side, *dout.shape), bf16),
            V((side, rows, half), bf16),
            V((side, rows, half), bf16),
            V((2, side, slots, half), bf16),
            V((2, side, slots, half), bf16),
            V((2, side, slots, half), bf16),
            V((2, part_rows, half), bf16),
            V((2, part_rows, half), bf16),
            V((2, side, slots, half), bf16),
            V((2, side, slots, half), bf16),
            V((side, rows, half), bf16),
            V((side, rows, half), bf16),
            V((3, rows, half), bf16),
            V((2, rows, half), bf16),
            V((rows, half), bf16),
            V((rows, half), bf16),
            V((rows, 128), f32),
            V((rows, 128), f32),
            V((2, part_rows, group * rows), bf16),
            V((2, group * rows, part_rows), bf16),
            V((side * rows, half), f32),
            pltpu.SemaphoreType.DMA((len(names),)),
            pltpu.SemaphoreType.DMA((kinds, side)),
            pltpu.SemaphoreType.DMA((kinds, side)),
            pltpu.SemaphoreType.DMA((5 + 2 * side,)),
            pltpu.SemaphoreType.DMA((5 + 2 * side,)),
        ],
        compiler_params=pltpu.CompilerParams(
            collective_id=0, has_side_effects=True, vmem_limit_bytes=VMEM_BYTES
        ),
        name="layer",
    )(*args.values())


def write_out(*refs):
    count = (len(refs) - 1) // 2
    copies = [
        pltpu.make_async_copy(refs[i], refs[count + i], refs[-1].at[i]) for i in range(count)
    ]
    for copy in copies:
        copy.start()
    for copy in copies:
        copy.wait()


def to_memory(*arrays):
    return pl.pallas_call(
        write_out,
        out_shape=tuple(jax.ShapeDtypeStruct(a.shape, a.dtype) for a in arrays),
        in_specs=[pl.BlockSpec(memory_space=pltpu.VMEM)] * len(arrays),
        out_specs=(pl.BlockSpec(memory_space=pltpu.HBM),) * len(arrays),
        scratch_shapes=[pltpu.SemaphoreType.DMA((len(arrays),))],
        name="write_out",
    )(*(pltpu.with_memory_space_constraint(a, pltpu.VMEM) for a in arrays))


def body(
    layer_input,
    ssm_state,
    w_input,
    decay_rate,
    frequency,
    step_log,
    input_map,
    output_map,
    skip_gain,
    glu_weight,
    mix_out,
    norm_gain,
    norm_shift,
    route_ids,
    route_weights,
    gate_expert,
    up_expert,
    down_expert,
    gate_shared,
    up_shared,
    down_shared,
    dense_in,
    dense_out,
    branch_gate,
    final_gain,
    final_shift,
):
    count_ep = lax.axis_size("ep")
    count_tp = lax.axis_size("tp")
    seq_rows, width = layer_input.shape
    top_k = route_ids.shape[1]
    experts = gate_expert.shape[0] * count_ep
    cap = count_tp * max(1, min(seq_rows // count_tp, seq_rows * top_k // experts))
    side = math.isqrt(count_ep)
    layer_output, new_state = layer(
        side,
        cap,
        experts,
        dict(
            ids=route_ids.T,
            scores=route_weights.T,
            rate=decay_rate,
            freq=frequency,
            step=step_log[None],
            imap=input_map.transpose(0, 1, 3, 2),
            omap=output_map,
            skip=skip_gain,
            x=layer_input,
            win=w_input,
            state=ssm_state.reshape(-1, ssm_state.shape[3]),
            din=dense_in,
            dout=dense_out,
            glu=glu_weight,
            mix=mix_out,
            gain=norm_gain[None],
            shift=norm_shift[None],
            gs=gate_shared,
            us=up_shared,
            ds=down_shared,
            ge=gate_expert[0],
            ue=up_expert[0],
            de=down_expert[0],
            bgate=branch_gate.reshape(-1, 128),
            fgain=final_gain[None],
            fshift=final_shift[None],
        ),
    )
    layer_output, new_state = to_memory(layer_output, new_state)
    new_state = new_state.reshape(ssm_state.shape)
    return (layer_output, new_state)


def solution(mesh):
    placed = (
        P(("grp", "ep"), None),
        P(None, ("grp", "ep"), "tp", None),
        P(None, "tp"),
        P("tp", None),
        P("tp", None),
        P("tp"),
        P(None, "tp", None, None),
        P(None, "tp", None, None),
        P("tp", None),
        P(),
        P(),
        P(),
        P(),
        P(("grp", "ep"), None),
        P(("grp", "ep"), None),
        P("ep", None, "tp"),
        P("ep", None, "tp"),
        P("ep", "tp", None),
        P(None, "tp"),
        P(None, "tp"),
        P("tp", None),
        P("ep", None),
        P("ep", "tp"),
        P(),
        P("tp"),
        P("tp"),
    )
    return jax.shard_map(
        body,
        mesh=mesh,
        in_specs=placed,
        out_specs=(P(("grp", "ep"), "tp"), P(None, ("grp", "ep"), "tp", None)),
        check_vma=False,
    )
```
